32 devices in a mesh: sp: 8 (over z, y), tp: 4 (over x, core).
Axes of the slice: x: 2, y: 2, z: 4, core: 2. Of those that a mesh axis runs over, the one named last changes fastest.
Arguments:
- queries: bfloat16 [4096, 1024], P('sp', 'tp'), may hold values from -6 to 6
- keys: bfloat16 [4096, 1024], P('sp', 'tp'), may hold values from -6 to 6
- values: bfloat16 [4096, 1024], P('sp', 'tp'), may hold values from -6 to 6
- cum_gate: float32 [4096, 16], P('sp', 'tp'), as said below
- documents: int32 [4096], P('sp'), may hold values from 0 to 3, never falling along the last dimension, each value on 1 to 2048 neighbouring positions
- head_gain: float32 [1024], P('tp'), may hold values from 0.1 to 1.9
- out_weight: bfloat16 [1024, 2048], replicated, may hold values from -0.1875 to 0.1875
- resid: bfloat16 [4096, 2048], P(('sp', 'tp')), may hold values from -6 to 6
- norm_gain: float32 [2048], replicated, may hold values from 0.1 to 1.9
- routes: int32 [4096, 2], P(('sp', 'tp')), may hold values from 0 to 7, all different within a row; in each aligned block of 128 rows (0 to 127, 128 to 255, ...) at most 64 rows name the same one
- route_weights: float32 [4096, 2], P(('sp', 'tp')), may hold values from 0.25 to 1
- w_gate: bfloat16 [8, 2048, 3584], P('sp', None, 'tp'), may hold values from -0.125 to 0.125
- w_up: bfloat16 [8, 2048, 3584], P('sp', None, 'tp'), may hold values from -0.125 to 0.125
- w_down: bfloat16 [8, 3584, 2048], P('sp', 'tp'), may hold values from -0.09375 to 0.09375
Outputs:
- mixed: bfloat16 [4096, 2048], P(('sp', 'tp'))
The draws below stay inside these ranges and needn't reach their ends.
Inputs may be any that keep to these rules, and one draw needn't show every extreme that they name: `cum_gate`: along the positions each head's values never rise. `documents`: document numbers never fall along the positions. `routes`: the 2 experts of a row differ. In each aligned block of 128 rows no expert is named more than 64 times; in some blocks an expert is named exactly 64 times.
All inputs are finite; a program needn't handle non-finite values.
Results may differ from the reference program's by a relative error of at most 0.015.
Values may be sent and summed in bfloat16 or wider, within the bound.
A program may use at most 128 MiB of HBM per device.

```python
import math
import jax
import jax.numpy as jnp
import numpy as np
from jax import lax

D = 2048
HEADS = 16
HEAD_DIM = 64
FFE = 3584
TOP = 2
TOK_DEV = 512
SEQUENCE_LENGTH = 4096
ROWS_DEV = 128
HD = 1024
EXPERTS = 8
CAP = 64
SLICE = 896
N_SP = 8
N_TP = 4


def draw_queries(key, part):
    drawn = jax.random.normal(jax.random.fold_in(key, 1), (SEQUENCE_LENGTH, HEADS * HEAD_DIM), jnp.float32)
    return jnp.clip(drawn, -6.0, 6.0).astype(jnp.bfloat16)


def draw_keys(key, part):
    drawn = jax.random.normal(jax.random.fold_in(key, 2), (SEQUENCE_LENGTH, HEADS * HEAD_DIM), jnp.float32)
    return jnp.clip(drawn, -6.0, 6.0).astype(jnp.bfloat16)


def draw_cum_gate(key, part):
    head_order = jax.random.permutation(jax.random.fold_in(key, 21), HEADS)
    fast_heads = head_order < HEADS // 2
    quick_decay_rate = jnp.exp(jax.random.uniform(jax.random.fold_in(key, 22), (HEADS,), jnp.float32, math.log(0.03), math.log(0.08)))
    slow_rate = jax.random.uniform(jax.random.fold_in(key, 23), (HEADS,), jnp.float32, 0.3, 0.8) / SEQUENCE_LENGTH
    head_rates = jnp.where(fast_heads, quick_decay_rate, slow_rate)
    blocks = SEQUENCE_LENGTH // TOK_DEV
    factor = jnp.exp(jax.random.uniform(jax.random.fold_in(key, 24), (blocks, HEADS), jnp.float32, -0.7, 0.7))
    factor = jnp.repeat(factor, TOK_DEV, axis=0)
    jitter = jax.random.uniform(jax.random.fold_in(key, 25), (SEQUENCE_LENGTH, HEADS), jnp.float32, 0.5, 1.5)
    logged_step_list = -head_rates[None, :] * factor * jitter
    spike_position = jax.random.randint(jax.random.fold_in(key, 26), (3,), 0, SEQUENCE_LENGTH)
    loss_values = jax.random.uniform(jax.random.fold_in(key, 27), (3, HEADS), jnp.float32, 0.2, 0.5)
    logged_step_list = logged_step_list.at[spike_position].add(jnp.log(1.0 - loss_values))
    return jnp.cumsum(logged_step_list, axis=0)


def block_scale(stream_key, shape, shards, smallest, high):
    factor_of = 1.0
    for axis_at, shards_of in shards:
        heights = jax.random.uniform(jax.random.fold_in(jax.random.fold_in(stream_key, 6), axis_at), (shards_of,), jnp.float32, smallest / len(shards), high / len(shards))
        factor_of = factor_of * jnp.repeat(jnp.exp(heights), shape[axis_at] // shards_of).reshape((-1,) + (1,) * (len(shape) - 1 - axis_at))
    return factor_of


def length_profile(count, total, reach, slope):
    loads = [(1 << 20) // math.isqrt(rank ** slope) + 1 for rank in range(2, count + 1)]
    spare, given = total - reach - (count - 1), [1] * (count - 1)
    while spare > 0:
        candidates = [i for i in range(count - 1) if given[i] < reach]
        pool, left = sum([loads[i] for i in candidates]), spare
        for i in candidates:
            addition = min(reach - given[i], max(1, left * loads[i] // pool), spare)
            given[i] = given[i] + addition
            spare = spare - addition
    return np.array([reach] + given)


def ragged_sizes(own_key, count, total, bound, lean):
    if count == 2:
        one = jax.random.randint(own_key, (), max(1, total - bound), min(bound, total - 1) + 1)
        return jnp.stack([one, total - one])
    sizes = jnp.asarray(length_profile(count, total, bound, lean), jnp.int32)
    twos = (count - 1) // 2
    source_of, taker = sizes[1:1 + 2 * twos:2], sizes[2:2 + 2 * twos:2]
    margin = jnp.minimum(source_of - 1, bound - taker)
    shifted = jax.random.randint(jax.random.fold_in(own_key, 1), (twos,), 0, 1 << 20) % (margin + 1)
    sizes = sizes.at[1:1 + 2 * twos:2].set(source_of - shifted).at[2:2 + 2 * twos:2].set(taker + shifted)
    return sizes[jax.random.permutation(jax.random.fold_in(own_key, 2), count)]


def shared_out(own_key, own, number, rows, count, top, most, lean):
    sequence = jax.random.permutation(own_key, count)
    heavy_load, usual = shares(count, rows * top, most, lean, True), shares(count, rows * top, most, lean, False)
    places = jnp.arange(count)

    def named(tallies, offset_by):
        used = int((tallies > 0).sum())
        fixed = max(1, used // 4)
        passed = fixed + (places - fixed + offset_by * (used - fixed)) % max(1, count - fixed)
        return jnp.zeros((count,), jnp.int32).at[sequence[jnp.where(places < fixed, places, passed)]].set(jnp.asarray(tallies, jnp.int32))

    tallies = jnp.where(number % 4 == 0, named(heavy_load, number // 4), named(usual, number - number // 4 - 1))
    mixed = jax.random.permutation(jax.random.fold_in(own, 3), count)
    source_of, sink = mixed[0:count // 2 * 2:2], mixed[1:count // 2 * 2:2]
    room = jnp.minimum(tallies[source_of] - 1, most - tallies[sink]) // 2
    room = jnp.where((source_of == sequence[0]) | (sink == sequence[0]) | (tallies[sink] == 0), 0, jnp.maximum(room, 0))
    passed = jax.random.randint(jax.random.fold_in(own, 4), (count // 2,), 0, 1 << 20) % (room + 1)
    tallies = tallies.at[source_of].add(-passed).at[sink].add(passed)
    labels = jnp.searchsorted(jnp.cumsum(tallies), jnp.arange(rows * top), side="right").astype(jnp.int32)
    table = labels.reshape(top, rows).T
    table = table[jax.random.permutation(jax.random.fold_in(own, 1), rows)]
    offset_by = jax.random.randint(jax.random.fold_in(own, 2), (rows, 1), 0, top)
    return jnp.take_along_axis(table, (jnp.arange(top)[None, :] + offset_by) % top, axis=1)


def shares(amount, total, limit, slope, full):
    portions = [(1 << 20) // math.isqrt(grade ** slope) + 1 for grade in range(1, amount + 1)]
    largest = limit if full else min(limit, max(-(-total // amount), total * portions[0] // sum(portions)))
    least = 1 if total - largest >= amount - 1 else 0
    counts, spare = [largest] + [least] * (amount - 1), total - largest - least * (amount - 1)
    while spare > 0:
        free = [i for i in range(1, amount) if counts[i] < largest] or [i for i in range(1, amount) if counts[i] < limit]
        whole, remaining = sum([portions[i] for i in free]), spare
        for i in free:
            extra = min(limit - counts[i], max(1, remaining * portions[i] // whole), spare)
            counts[i] = counts[i] + extra
            spare = spare - extra
    return np.array(counts)


def noise(stream_key, dims, spread, bound, split=(), held_as=jnp.bfloat16):
    entries = jax.random.normal(stream_key, dims, jnp.float32) * spread
    if len(split) > 0:
        entries = block_scale(stream_key, dims, split, -0.22, 0.18) * entries
    return jnp.clip(entries, min=-bound, max=bound).astype(held_as)


def setup_inputs(seed: int = 0) -> dict:
    seeds = jax.random.split(jax.random.key(seed), 15)
    queries = draw_queries(jax.random.fold_in(seeds[14], 71), 0)
    keys = draw_keys(jax.random.fold_in(seeds[14], 71), 0)
    values = noise(seeds[2], (SEQUENCE_LENGTH, HD), 1.0, 6.0, ((0, 8), (1, 4)))
    cum_gate = draw_cum_gate(jax.random.fold_in(seeds[14], 71), 0)
    documents = jnp.searchsorted(jnp.cumsum(ragged_sizes(seeds[4], 4, SEQUENCE_LENGTH, SEQUENCE_LENGTH // 2, 2)), jnp.arange(SEQUENCE_LENGTH), side="right").astype(jnp.int32)
    head_gain = jnp.clip(1.0 + 0.18 * jax.random.normal(seeds[5], (HD,), jnp.float32), 0.1, 1.9)
    out_weight = noise(seeds[6], (HD, D), HD ** -0.5, 0.1875)
    resid = noise(seeds[7], (SEQUENCE_LENGTH, D), 1.0, 6.0, ((0, 32),))
    norm_gain = jnp.clip(1.0 + 0.18 * jax.random.normal(seeds[8], (D,), jnp.float32), 0.1, 1.9)
    routes_keys = jax.random.split(jax.random.fold_in(seeds[9], 1), SEQUENCE_LENGTH // ROWS_DEV)
    routes_turns = jax.random.permutation(jax.random.fold_in(seeds[9], 3), SEQUENCE_LENGTH // ROWS_DEV)
    routes = jax.vmap(lambda own, number: shared_out(jax.random.fold_in(seeds[9], 2), own, number, ROWS_DEV, EXPERTS, TOP, CAP, 2))(routes_keys, routes_turns).reshape((SEQUENCE_LENGTH, TOP))
    route_weights = jnp.clip(jnp.exp(math.log(1.0) - 1.3862944 * jax.random.uniform(seeds[10], (SEQUENCE_LENGTH, TOP), jnp.float32) ** block_scale(seeds[10], (SEQUENCE_LENGTH, TOP), ((0, 32),), -0.2, 0.2)), 0.25, 1.0)
    w_gate = noise(seeds[11], (EXPERTS, D, FFE), D ** -0.5, 0.125, ((0, 8), (2, 4)))
    w_up = noise(seeds[12], (EXPERTS, D, FFE), D ** -0.5, 0.125, ((0, 8), (2, 4)))
    w_down = noise(seeds[13], (EXPERTS, FFE, D), FFE ** -0.5, 0.09375, ((0, 8), (1, 4)))
    return dict(queries=queries, keys=keys, values=values, cum_gate=cum_gate, documents=documents, head_gain=head_gain, out_weight=out_weight, resid=resid, norm_gain=norm_gain, routes=routes, route_weights=route_weights, w_gate=w_gate, w_up=w_up, w_down=w_down)


EPS = 1e-06

def attention(queries, keys, values, cum_gate, documents):
    block_len = math.gcd(SEQUENCE_LENGTH, 256)
    block_count = SEQUENCE_LENGTH // block_len
    key_heads = keys.reshape(SEQUENCE_LENGTH, HEADS, HEAD_DIM).astype(jnp.float32)
    value_heads = values.reshape(SEQUENCE_LENGTH, HEADS, HEAD_DIM).astype(jnp.float32)
    positions = jnp.arange(SEQUENCE_LENGTH, dtype=jnp.int32)
    score_scale = HEAD_DIM ** (-0.5)

    def one_block(block_index):
        first_pos = block_index * block_len
        query_row_block = lax.dynamic_slice_in_dim(queries, first_pos, block_len, 0)
        query_row_block = query_row_block.reshape(block_len, HEADS, HEAD_DIM).astype(jnp.float32)
        gate_here = lax.dynamic_slice_in_dim(cum_gate, first_pos, block_len, 0)
        doc_here = lax.dynamic_slice_in_dim(documents, first_pos, block_len, 0)
        query_pos = first_pos + jnp.arange(block_len, dtype=jnp.int32)
        scores = jnp.einsum('qhd,khd->qhk', query_row_block, key_heads) * score_scale
        scores = scores + gate_here[:, :, None] - cum_gate.T[None, :, :]
        allowed = (positions[None, :] <= query_pos[:, None]) & (documents[None, :] == doc_here[:, None])
        scores = jnp.where(allowed[:, None, :], scores, -jnp.inf)
        row_max = lax.optimization_barrier(jnp.max(scores, axis=-1, keepdims=True))
        exp_scores = jnp.exp(scores - row_max)
        row_sum = lax.optimization_barrier(jnp.sum(exp_scores, axis=-1))
        weights = lax.optimization_barrier(exp_scores.astype(jnp.bfloat16)).astype(jnp.float32)
        return jnp.einsum('qhk,khd->qhd', weights, value_heads) / row_sum[:, :, None]
    attended = lax.map(one_block, jnp.arange(block_count, dtype=jnp.int32))
    return attended.reshape(SEQUENCE_LENGTH, HEADS, HEAD_DIM)

def experts_out(expert_input, routes, w_gate, w_up, w_down):
    capacity = N_SP * N_TP * CAP
    flat_routes = routes.reshape(-1)
    route_total = flat_routes.shape[0]
    owners = jnp.arange(route_total, dtype=jnp.int32) // TOP

    def one_expert(expert_index):
        matches = (flat_routes == expert_index).astype(jnp.int32)
        ranks = jnp.cumsum(matches) - 1
        slots = jnp.where(matches == 1, ranks, capacity)
        slot_owner = jnp.zeros((capacity + 1,), jnp.int32).at[slots].set(owners)[:capacity]
        picked = expert_input[slot_owner]
        gate_out = jnp.dot(picked, w_gate[expert_index], preferred_element_type=jnp.float32)
        up_out = jnp.dot(picked, w_up[expert_index], preferred_element_type=jnp.float32)
        hidden = (jax.nn.silu(gate_out) * up_out).astype(jnp.bfloat16)
        pieces = hidden.reshape(capacity, N_TP, SLICE).astype(jnp.float32)
        down_blocks = w_down[expert_index].reshape(N_TP, SLICE, D).astype(jnp.float32)
        partial_value = jnp.einsum('rjf,jfd->jrd', pieces, down_blocks)
        partial_value = lax.optimization_barrier(partial_value.astype(jnp.bfloat16)).astype(jnp.float32)
        return lax.optimization_barrier(jnp.sum(partial_value, axis=0)).astype(jnp.bfloat16)
    results = lax.map(one_expert, jnp.arange(EXPERTS, dtype=jnp.int32))
    onehot = (flat_routes[:, None] == jnp.arange(EXPERTS, dtype=jnp.int32)[None, :]).astype(jnp.int32)
    ranks = lax.optimization_barrier(jnp.sum(jnp.cumsum(onehot, axis=0) * onehot, axis=1)) - 1
    return results[flat_routes, ranks].reshape(SEQUENCE_LENGTH, TOP, D)

def reference(queries, keys, values, cum_gate, documents, head_gain, out_weight, resid, norm_gain, routes, route_weights, w_gate, w_up, w_down):
    attended = attention(queries, keys, values, cum_gate, documents)
    mean_square = lax.optimization_barrier(jnp.mean(attended * attended, axis=-1, keepdims=True))
    head_normed = (attended * lax.rsqrt(mean_square + EPS)).reshape(SEQUENCE_LENGTH, HEADS * HEAD_DIM) * head_gain
    head_normed = head_normed.astype(jnp.bfloat16)
    projected = jnp.dot(head_normed, out_weight, preferred_element_type=jnp.float32)
    stream = lax.optimization_barrier((resid.astype(jnp.float32) + projected).astype(jnp.bfloat16))
    widened = stream.astype(jnp.float32)
    mean_wide = lax.optimization_barrier(jnp.mean(widened * widened, axis=-1, keepdims=True))
    expert_input = (widened * lax.rsqrt(mean_wide + EPS) * norm_gain).astype(jnp.bfloat16)
    gathered = experts_out(expert_input, routes, w_gate, w_up, w_down)
    mixed = widened + lax.optimization_barrier(jnp.sum(route_weights[:, :, None] * gathered.astype(jnp.float32), axis=1))
    return mixed.astype(jnp.bfloat16)
```

```python
import functools

import jax
import jax.numpy as jnp
from jax import lax
from jax.experimental import pallas as pl
from jax.experimental.pallas import tpu as pltpu
from jax.sharding import PartitionSpec as P

EPS = 1e-06
MESH = pl.DeviceIdType.MESH
NEG = -1e30
VMEM_LIMIT = 65000 * 1024
LANES = 128
SPLITS = 2
BF = jnp.bfloat16
F32 = jnp.float32


def layer_kernel(
    n,
    head_size,
    cap,
    q_hbm,
    k_hbm,
    v_hbm,
    aux_ref,
    gain_ref,
    wo_hbm,
    resid_hbm,
    norm_gain_ref,
    routes_ref,
    routes_t_ref,
    route_w_ref,
    wg_hbm,
    wu_hbm,
    wd_hbm,
    mixed_ref,
    q_in,
    qs,
    kv,
    aux_all,
    top,
    acc,
    normed,
    gathered,
    wo,
    resid,
    wide,
    xin,
    into,
    out_ref,
    ret_ref,
    fan,
    wg,
    wu,
    wd,
    hidden,
    part,
    got,
    pair,
    across,
    fin,
    in_sem,
    kv_sem,
    w_sem,
    own_sem,
    up_send,
    up_recv,
    over_send,
    over_recv,
    aux_send,
    aux_recv,
    h_send,
    h_recv,
    a_send,
    a_recv,
    x_send,
    x_recv,
    c_send,
    c_recv,
    d_send,
    d_recv,
    p_send,
    p_recv,
    s_send,
    s_recv,
    r_send,
    r_recv,
):
    me = lax.axis_index("sp")
    t = lax.axis_index("tp")
    c, xi = lax.rem(t, 2), t // 2
    near = xi * 2 + (1 - c)
    far = (1 - xi) * 2 + c
    diag = 3 - t
    y, z = lax.rem(me, 2), me // 2
    floors, reach = n // 2, n // 4
    near_id = {"sp": me, "tp": near}
    far_id = {"sp": me, "tp": far}
    diag_id = {"sp": me, "tp": diag}
    mate_id = {"sp": me + 1 - 2 * y, "tp": t}
    above_id = {"sp": lax.rem(me + 2, n), "tp": t}

    tokens, width_here = q_in.shape
    pairs = width_here // LANES
    hpp = LANES // head_size
    keys = tokens // SPLITS
    chunks = pairs * SPLITS
    rows, width = mixed_ref.shape

    loads = [
        pltpu.make_async_copy(
            src.at[pl.ds(s * keys, keys), pl.ds(p * LANES, LANES)],
            kv.at[0, p * SPLITS + s, j],
            kv_sem.at[(p * SPLITS + s) * 2 + j],
        )
        for p in range(pairs)
        for s in range(SPLITS)
        for j, src in enumerate((k_hbm, v_hbm))
    ]
    q_load = pltpu.make_async_copy(q_hbm, q_in, in_sem.at[0])
    wo_load = pltpu.make_async_copy(wo_hbm, wo, in_sem.at[1])
    resid_load = pltpu.make_async_copy(resid_hbm, resid, in_sem.at[2])
    weights = [
        pltpu.make_async_copy(src, dst, w_sem.at[i])
        for i, (src, dst) in enumerate(((wg_hbm, wg), (wu_hbm, wu), (wd_hbm, wd)))
    ]
    for copy in loads:
        copy.start()
    q_load.start()

    barrier = pltpu.get_barrier_semaphore()

    def greet(k, carry):
        pl.semaphore_signal(
            barrier,
            inc=1,
            device_id={"sp": lax.rem(me + k, n), "tp": t},
            device_id_type=MESH,
        )
        return carry

    lax.fori_loop(1, n, greet, 0)
    for other in (near_id, far_id, diag_id):
        pl.semaphore_signal(barrier, inc=1, device_id=other, device_id_type=MESH)

    def remote(src, dst, send, recv, to):
        return pltpu.make_async_remote_copy(
            src_ref=src, dst_ref=dst, send_sem=send, recv_sem=recv, device_id=to, device_id_type=MESH
        )

    def up(d, i):
        return remote(
            kv.at[d, i],
            kv.at[d + 1, i],
            up_send.at[d * chunks + i],
            up_recv.at[d * chunks + i],
            above_id,
        )

    def over(d, i):
        return remote(
            kv.at[d, i],
            kv.at[reach + 1 + d, i],
            over_send.at[d * chunks + i],
            over_recv.at[d * chunks + i],
            mate_id,
        )

    def aux_copy(k):
        return remote(
            aux_ref,
            aux_all.at[k],
            aux_send.at[k],
            aux_recv.at[k],
            {"sp": lax.rem(me + k, n), "tp": t},
        )

    def rising(d):
        return (z + 1 < floors) & (z >= d) & (d < reach)

    def crossing(d):
        return (z >= d) & ((d > 0) | (y == 0)) & ((d < reach) | (y == 1))

    def coming(d):
        return (z >= d) & ((d > 0) | (y == 1)) & ((d < reach) | (y == 0))

    def forward(d, i):
        @pl.when(rising(d))
        def _():
            up(d, i).start()

        @pl.when(crossing(d))
        def _():
            over(d, i).start()

    for copy in loads:
        copy.wait()
    pl.semaphore_wait(barrier, n + 2)
    lax.fori_loop(0, chunks, lambda i, z_: (forward(0, i), z_)[1], 0)

    def send_aux(k, carry):
        @pl.when(me + k < n)
        def _():
            aux_copy(k).start()

        return carry

    lax.fori_loop(1, n // 2 + 1, send_aux, 0)
    wo_load.start()
    resid_load.start()
    for copy in weights:
        copy.start()

    lane = lax.broadcasted_iota(jnp.int32, (1, LANES), 1)
    tile = min(tokens, 256)

    def mine(h):
        return (lane >= h * head_size) & (lane < (h + 1) * head_size)

    q_load.wait()
    for p in range(pairs):
        block = q_in[:, p * LANES : (p + 1) * LANES].astype(F32) * (head_size ** (-0.5))
        for h in range(hpp):
            qs[p, h] = jnp.where(mine(h), block, 0.0).astype(BF)
    top[...] = jnp.full(top.shape, NEG, F32)
    acc[...] = jnp.zeros(acc.shape, F32)

    def wider(x):
        return jnp.concatenate([x] * (keys // LANES), axis=1) if keys > LANES else x[:, :keys]

    def visit(slot, i, p, h, r0, bias, allowed):
        at = pl.ds(r0, tile)
        k = kv[slot, i, 0]
        v = jnp.where(mine(h), kv[slot, i, 1].astype(F32), 1.0).astype(BF)
        scores = lax.dot_general(
            qs[p, h, at, :], k, (((1,), (1,)), ((), ())), preferred_element_type=F32
        )
        scores = scores + bias
        if allowed is not None:
            scores = jnp.where(allowed, scores, NEG)
        before = top[p, h, at, :]
        highest = jnp.maximum(before, jnp.max(scores, axis=1, keepdims=True))
        exps = jnp.exp(scores - wider(highest))
        rescale = jnp.exp(before - highest)
        top[p, h, at, :] = highest
        acc[p, h, at, :] = acc[p, h, at, :] * rescale + jnp.dot(
            exps.astype(BF), v, preferred_element_type=F32
        )

    first_doc = aux_ref[0][hpp : hpp + 1, 0:1]
    spots_r = lax.broadcasted_iota(jnp.int32, (keys, keys), 0)
    spots_c = lax.broadcasted_iota(jnp.int32, (keys, keys), 1)
    doc_cols = [
        jnp.sum(
            jnp.where(spots_r == spots_c, aux_ref[s][hpp : hpp + 1, :], 0.0), axis=1, keepdims=True
        )
        for s in range(SPLITS)
    ]
    doc_col = jnp.concatenate(doc_cols, axis=0)

    def diagonal(p, carry):
        for s in range(SPLITS):
            i = p * SPLITS + s
            side = aux_ref[i]
            for h in range(hpp):
                base = aux_ref[p * SPLITS][h : h + 1, 0:1]
                bias = base - side[h : h + 1, :]
                for r0 in range(0, tokens, tile):
                    if r0 + tile <= s * keys:
                        continue
                    key_pos = s * keys + lax.broadcasted_iota(jnp.int32, (1, keys), 1)
                    query_pos = r0 + lax.broadcasted_iota(jnp.int32, (tile, 1), 0)
                    allowed = (key_pos <= query_pos) & (
                        side[hpp : hpp + 1, :] == doc_col[r0 : r0 + tile]
                    )
                    visit(0, i, p, h, r0, bias, allowed)
        return carry

    lax.fori_loop(0, pairs, diagonal, 0)
    shut = jnp.where(doc_col == first_doc, 0.0, 2e30)
    for p in range(pairs):
        for h in range(hpp):
            top[p, h] = jnp.where(shut > 0.0, 1e30, top[p, h])

    def earlier(slot, dist, i):
        p = i // SPLITS
        side = aux_all[dist, i]
        zero = aux_ref[p * SPLITS]
        for h in range(hpp):
            bias = jnp.where(
                side[hpp : hpp + 1, :] == first_doc, zero[h : h + 1, 0:1] - side[h : h + 1, :], NEG
            )
            for r0 in range(0, tokens, tile):
                visit(slot, i, p, h, r0, bias, None)

    def aux_here(k, i):
        @pl.when(i == 0)
        def _():
            aux_copy(k).wait_recv()

    def crossed(d, i):
        @pl.when(coming(d))
        def _():
            dist = 2 * d + 2 * y - 1
            aux_here(dist, i)
            over(d, i).wait_recv()
            earlier(reach + 1 + d, dist, i)

    def history(j, carry):
        d, i = j // chunks + 1, lax.rem(j, chunks)

        @pl.when(z >= d)
        def _():
            up(d - 1, i).wait_recv()
            forward(d, i)
            aux_here(2 * d, i)
            earlier(d, 2 * d, i)

        crossed(d - 1, i)
        return carry

    lax.fori_loop(0, reach * chunks, history, 0)
    lax.fori_loop(0, chunks, lambda i, z_: (crossed(reach, i), z_)[1], 0)

    def h_copy(q, to):
        return remote(normed.at[q], gathered.at[t], h_send.at[q], h_recv.at[t], to)

    def h_in(q):
        return remote(normed.at[q], gathered.at[q], h_send.at[q], h_recv.at[q], near_id)

    def settle(q):
        at = pl.ds(pl.multiple_of(q * rows, rows), rows)
        for p in range(pairs):
            total = None
            for h in range(hpp):
                state = acc[p, h, at, :]
                sums = pltpu.roll(state, head_size, 1)
                attended = jnp.where(mine(h), state / sums, 0.0)
                mean_square = jnp.sum(attended * attended, axis=1, keepdims=True) / head_size
                piece = attended * lax.rsqrt(mean_square + EPS)
                total = piece if total is None else total + piece
            cols = slice(p * LANES, (p + 1) * LANES)
            normed[q, :, cols] = (total * gain_ref[:, cols]).astype(BF)

    for q, to in ((far, far_id), (diag, diag_id), (near, near_id)):
        settle(q)
        h_copy(q, to).start()
    settle(t)

    wide_tile = 512 if width % 512 == 0 else width
    experts = lax.broadcasted_iota(jnp.int32, (max(n, 8), 1), 0)
    named_t = (routes_t_ref[0:1, :] == experts) | (routes_t_ref[1:2, :] == experts)
    row_r = lax.broadcasted_iota(jnp.int32, (rows, rows), 0)
    row_c = lax.broadcasted_iota(jnp.int32, (rows, rows), 1)
    named_t = named_t.astype(F32)
    ranks_t = jnp.dot(
        named_t.astype(BF), (row_r < row_c).astype(F32).astype(BF), preferred_element_type=F32
    )
    ranks_t = jnp.where(named_t > 0.0, ranks_t, -1.0)
    slots = lax.broadcasted_iota(jnp.int32, (cap, 1), 0).astype(F32)
    for e in range(n):
        into[e * cap : (e + 1) * cap, :] = jnp.where(
            ranks_t[e : e + 1, :] == slots, 1.0, 0.0
        ).astype(BF)
    first_e, second_e = routes_ref[:, 0:1], routes_ref[:, 1:2]
    named = ((first_e == lane) | (second_e == lane)).astype(F32)
    ranks = jnp.dot(
        (row_c < row_r).astype(F32).astype(BF), named.astype(BF), preferred_element_type=F32
    )
    wants = []
    for e in (first_e, second_e):
        rank = jnp.sum(jnp.where(e == lane, ranks, 0.0), axis=1, keepdims=True)
        wants.append(e.astype(F32) * cap + rank)
    wants = jnp.concatenate(wants, axis=0)

    wo_load.wait()
    resid_load.wait()

    def product(src, q, at):
        return jnp.dot(
            src,
            wo[pl.ds(pl.multiple_of(q * width_here, width_here), width_here), at : at + wide_tile],
            preferred_element_type=F32,
        )

    for at in range(0, width, wide_tile):
        wide[:, at : at + wide_tile] = product(normed[t], t, at)
    h_in(near).wait_recv()
    for at in range(0, width, wide_tile):
        wide[:, at : at + wide_tile] += product(gathered[near], near, at)
    h_in(far).wait_recv()
    h_in(diag).wait_recv()
    squares = jnp.zeros((rows, 1), F32)
    for at in range(0, width, wide_tile):
        cols = slice(at, at + wide_tile)
        value = (
            wide[:, cols]
            + product(gathered[far], far, at)
            + product(gathered[diag], diag, at)
            + resid[:, cols].astype(F32)
        )
        value = value.astype(BF).astype(F32)
        wide[:, cols] = value
        squares = squares + jnp.sum(value * value, axis=1, keepdims=True)
    scale = lax.rsqrt(squares / width + EPS)
    for at in range(0, width, wide_tile):
        cols = slice(at, at + wide_tile)
        xin[:, cols] = (wide[:, cols] * scale * norm_gain_ref[:, cols]).astype(BF)
    for at in range(0, width, wide_tile):
        cols = slice(at, at + wide_tile)
        sent = jnp.dot(into[...], xin[:, cols], preferred_element_type=F32).astype(BF)
        for e in range(n):
            out_ref[e, :, cols] = sent[e * cap : (e + 1) * cap]

    def source(k):
        return lax.rem(me - k + n, n)

    def a_out(k):
        to = lax.rem(me + k, n)
        return remote(
            out_ref.at[to], fan.at[me, t], a_send.at[k], a_recv.at[me], {"sp": to, "tp": t}
        )

    def a_in(k):
        p = source(k)
        return remote(out_ref.at[p], fan.at[p, t], a_send.at[k], a_recv.at[p], near_id)

    def x_copy(k, q):
        p = source(k)
        return remote(fan.at[p, q], fan.at[p, q], x_send.at[p], x_recv.at[p], far_id)

    def c_copy(k, q):
        p = source(k)
        return remote(fan.at[p, q], fan.at[p, q], c_send.at[p], c_recv.at[p], near_id)

    def d_copy(k, q):
        p = source(k)
        return remote(fan.at[p, q], fan.at[p, q], d_send.at[p], d_recv.at[p], near_id)

    def p_copy(k):
        p = source(k)
        return remote(part.at[p, 1 - c], got.at[p], p_send.at[p], p_recv.at[p], near_id)

    def s_copy(k):
        p = source(k)
        return remote(pair.at[p], across.at[p], s_send.at[p], s_recv.at[p], far_id)

    def r_out(k):
        p = source(k)
        return remote(fin.at[p], ret_ref.at[me], r_send.at[p], r_recv.at[me], {"sp": p, "tp": t})

    def r_in(k):
        p = source(k)
        return remote(fin.at[p], ret_ref.at[p], r_send.at[p], r_recv.at[p], near_id)

    own = pltpu.make_async_copy(out_ref.at[me], fan.at[me, t], own_sem)
    own.start()
    lax.fori_loop(1, n, lambda k, z_: (a_out(k).start(), z_)[1], 0)

    def spread(k):
        x_copy(k, t).start()
        c_copy(k, t).start()

    own.wait()
    spread(0)

    def step_a(k):
        a_in(k).wait_recv()
        spread(k)

    def step_x(k):
        x_copy(k, far).wait_recv()
        d_copy(k, far).start()

    def step_compute(k):
        p = source(k)
        c_copy(k, near).wait_recv()
        d_copy(k, diag).wait_recv()
        block = fan[p].reshape(4 * cap, width)
        gate = jnp.dot(block, wg[...], preferred_element_type=F32)
        up_ = jnp.dot(block, wu[...], preferred_element_type=F32)
        hidden[...] = (gate * jax.nn.sigmoid(gate) * up_).astype(BF)
        for at in range(0, width, wide_tile):
            down = jnp.dot(
                hidden[...], wd[:, at : at + wide_tile], preferred_element_type=F32
            ).astype(BF)
            for q in range(4):
                part[p, q % 2, q // 2, :, at : at + wide_tile] = down[q * cap : (q + 1) * cap]
        p_copy(k).start()

    def step_pair(k):
        p = source(k)
        p_copy(k).wait_recv()
        pair[p] = (part[p, c, 1 - xi].astype(F32) + got[p, 1 - xi].astype(F32)).astype(BF)
        s_copy(k).start()

    def step_final(k):
        p = source(k)
        s_copy(k).wait_recv()
        total = (
            part[p, c, xi].astype(F32) + got[p, xi].astype(F32) + across[p].astype(F32)
        ).astype(BF)

        @pl.when(k == 0)
        def _():
            ret_ref[me] = total

        @pl.when(k > 0)
        def _():
            fin[p] = total
            r_out(k).start()

    step_a(1)
    step_x(0)
    for copy in weights:
        copy.wait()

    def iteration(i, carry):
        @pl.when(i + 2 < n)
        def _():
            step_a(i + 2)

        @pl.when(i + 1 < n)
        def _():
            step_x(i + 1)

        @pl.when((i >= 1) & (i < n + 1))
        def _():
            step_pair(i - 1)

        @pl.when(i < n)
        def _():
            step_compute(i)

        @pl.when(i >= 2)
        def _():
            step_final(i - 2)

        return carry

    lax.fori_loop(0, n + 2, iteration, 0)

    slot = lax.broadcasted_iota(jnp.int32, (1, cap), 1)

    def combine(p):
        picks = (wants == (p * cap + slot).astype(F32)).astype(F32).astype(BF)
        for at in range(0, width, wide_tile):
            cols = slice(at, at + wide_tile)
            chosen = jnp.dot(picks, ret_ref[p, :, cols], preferred_element_type=F32)
            wide[:, cols] += (
                route_w_ref[:, 0:1] * chosen[:rows] + route_w_ref[:, 1:2] * chosen[rows:]
            )

    combine(me)

    def gather(i, carry):
        k = n - 1 - i
        r_in(k).wait_recv()
        combine(source(k))
        return carry

    lax.fori_loop(0, n - 1, gather, 0)
    mixed_ref[...] = wide[...].astype(BF)

    def sent_history(j, carry):
        d, i = j // chunks, lax.rem(j, chunks)

        @pl.when(rising(d))
        def _():
            up(d, i).wait_send()

        @pl.when(crossing(d))
        def _():
            over(d, i).wait_send()

        return carry

    lax.fori_loop(0, (reach + 1) * chunks, sent_history, 0)

    def sent_aux(k, carry):
        @pl.when(me + k < n)
        def _():
            aux_copy(k).wait_send()

        return carry

    lax.fori_loop(1, n // 2 + 1, sent_aux, 0)
    for q, to in ((far, far_id), (diag, diag_id), (near, near_id)):
        h_copy(q, to).wait_send()

    def finish(k, carry):
        x_copy(k, t).wait_send()
        c_copy(k, t).wait_send()
        d_copy(k, far).wait_send()
        p_copy(k).wait_send()
        s_copy(k).wait_send()

        @pl.when(k > 0)
        def _():
            a_out(k).wait_send()
            r_out(k).wait_send()

        return carry

    lax.fori_loop(0, n, finish, 0)


def on_device(
    queries,
    keys,
    values,
    cum_gate,
    documents,
    head_gain,
    out_weight,
    resid,
    norm_gain,
    routes,
    route_weights,
    w_gate,
    w_up,
    w_down,
):
    tokens, width_here = queries.shape
    heads_here = cum_gate.shape[1]
    head_size = width_here // heads_here
    n = lax.axis_size("sp")
    tp_count = lax.axis_size("tp")
    rows, width = resid.shape
    top_count = routes.shape[1]
    cap = 2 * top_count * tokens // (tp_count * n)
    hid = w_gate.shape[2]
    pairs, hpp = width_here // LANES, LANES // head_size
    part_len = tokens // SPLITS
    chunks = pairs * SPLITS
    reach = n // 4

    gates = cum_gate.T.reshape(pairs, hpp, SPLITS, part_len).transpose(0, 2, 1, 3)
    docs = jnp.broadcast_to(
        documents.astype(F32).reshape(1, SPLITS, 1, part_len), (pairs, SPLITS, 8 - hpp, part_len)
    )
    aux = jnp.concatenate([gates, docs], axis=2).reshape(chunks, 8, part_len)

    dma = pltpu.SemaphoreType.DMA
    hbm = pl.BlockSpec(memory_space=pl.ANY)
    vmem = pl.BlockSpec(memory_space=pltpu.VMEM)
    return pl.pallas_call(
        functools.partial(layer_kernel, n, head_size, cap),
        out_shape=jax.ShapeDtypeStruct((rows, width), BF),
        in_specs=[hbm] * 3 + [vmem] * 2 + [hbm] * 2 + [vmem] * 4 + [hbm] * 3,
        out_specs=vmem,
        scratch_shapes=[
            pltpu.VMEM((tokens, width_here), BF),
            pltpu.VMEM((pairs, hpp, tokens, LANES), BF),
            pltpu.VMEM((2 * reach + 2, chunks, 2, part_len, LANES), BF),
            pltpu.VMEM((n // 2 + 1, chunks, 8, part_len), F32),
            pltpu.VMEM((pairs, hpp, tokens, LANES), F32),
            pltpu.VMEM((pairs, hpp, tokens, LANES), F32),
            pltpu.VMEM((tp_count, rows, width_here), BF),
            pltpu.VMEM((tp_count, rows, width_here), BF),
            pltpu.VMEM((tp_count * width_here, width), BF),
            pltpu.VMEM((rows, width), BF),
            pltpu.VMEM((rows, width), F32),
            pltpu.VMEM((rows, width), BF),
            pltpu.VMEM((n * cap, rows), BF),
            pltpu.VMEM((n, cap, width), BF),
            pltpu.VMEM((n, cap, width), BF),
            pltpu.VMEM((n, 4, cap, width), BF),
            pltpu.VMEM((width, hid), BF),
            pltpu.VMEM((width, hid), BF),
            pltpu.VMEM((hid, width), BF),
            pltpu.VMEM((4 * cap, hid), BF),
            pltpu.VMEM((n, 2, 2, cap, width), BF),
            pltpu.VMEM((n, 2, cap, width), BF),
            pltpu.VMEM((n, cap, width), BF),
            pltpu.VMEM((n, cap, width), BF),
            pltpu.VMEM((n, cap, width), BF),
            dma((3,)),
            dma((2 * chunks,)),
            dma((3,)),
            dma,
        ]
        + [dma(((reach + 1) * chunks,)) for _ in range(4)]
        + [dma((n // 2 + 1,)) for _ in range(2)]
        + [dma((tp_count,)) for _ in range(2)]
        + [dma((n,)) for _ in range(14)],
        compiler_params=pltpu.CompilerParams(
            collective_id=1, has_side_effects=True, vmem_limit_bytes=VMEM_LIMIT
        ),
    )(
        queries,
        keys,
        values,
        aux,
        head_gain[None, :],
        out_weight,
        resid,
        norm_gain[None, :],
        routes,
        routes.T,
        route_weights,
        w_gate[0],
        w_up[0],
        w_down[0],
    )


def solution(mesh):
    in_specs = (
        P("sp", "tp"),
        P("sp", "tp"),
        P("sp", "tp"),
        P("sp", "tp"),
        P("sp"),
        P("tp"),
        P(),
        P(("sp", "tp"), None),
        P(),
        P(("sp", "tp"), None),
        P(("sp", "tp"), None),
        P("sp", None, "tp"),
        P("sp", None, "tp"),
        P("sp", "tp", None),
    )
    out_specs = P(("sp", "tp"), None)
    return jax.shard_map(
        on_device, mesh=mesh, in_specs=in_specs, out_specs=out_specs, check_vma=False
    )
```

```python
import functools

import jax
import jax.numpy as jnp
from jax import lax
from jax.experimental import pallas as pl
from jax.experimental.pallas import tpu as pltpu
from jax.sharding import PartitionSpec as P

EPS = 1e-06
MESH = pl.DeviceIdType.MESH
NEG = -1e30
VMEM_LIMIT = 67043328
LANES = 128
SPLITS = 2
BF = jnp.bfloat16
F32 = jnp.float32


def layer_kernel(
    n,
    head_size,
    cap,
    q_hbm,
    k_hbm,
    v_hbm,
    gates_ref,
    docs_ref,
    gain_ref,
    wo_hbm,
    resid_hbm,
    norm_gain_ref,
    routes_ref,
    route_w_ref,
    wg_hbm,
    wu_hbm,
    wd_hbm,
    mixed_ref,
    q_in,
    qs,
    kv,
    aux_ref,
    aux_all,
    route_own,
    route_all,
    top,
    acc,
    normed,
    gathered,
    wo,
    wide,
    raw,
    crossing_rows,
    ret_ref,
    fan,
    wg,
    wu,
    wd,
    hidden,
    part,
    got,
    across,
    in_sem,
    kv_sem,
    w_sem,
    up_send,
    up_recv,
    over_send,
    over_recv,
    aux_send,
    aux_recv,
    h_send,
    h_recv,
    route_send,
    route_recv,
    rise_send,
    fall_send,
    raw_recv,
    y_send,
    y_recv,
    x_send,
    x_recv,
    c_send,
    c_recv,
    d_send,
    d_recv,
    p_send,
    p_recv,
    s_send,
    s_recv,
    r_send,
    r_recv,
):
    me = lax.axis_index("sp")
    t = lax.axis_index("tp")
    c, xi = lax.rem(t, 2), t // 2
    near = xi * 2 + (1 - c)
    far = (1 - xi) * 2 + c
    diag = 3 - t
    y, z = lax.rem(me, 2), me // 2
    floors, reach = n // 2, n // 4
    near_id = {"sp": me, "tp": near}
    far_id = {"sp": me, "tp": far}
    diag_id = {"sp": me, "tp": diag}
    mate_id = {"sp": me + 1 - 2 * y, "tp": t}
    above_id = {"sp": lax.rem(me + 2, n), "tp": t}
    below_id = {"sp": lax.rem(me + n - 2, n), "tp": t}

    tokens, width_here = q_in.shape
    pairs = width_here // LANES
    hpp = LANES // head_size
    keys = tokens // SPLITS
    chunks = pairs * SPLITS
    rows, width = mixed_ref.shape

    loads = [
        pltpu.make_async_copy(
            src.at[pl.ds(s * keys, keys), pl.ds(p * LANES, LANES)],
            kv.at[0, p * SPLITS + s, j],
            kv_sem.at[(p * SPLITS + s) * 2 + j],
        )
        for p in range(pairs)
        for s in range(SPLITS)
        for j, src in enumerate((k_hbm, v_hbm))
    ]
    q_load = pltpu.make_async_copy(q_hbm, q_in, in_sem.at[0])
    wo_load = pltpu.make_async_copy(wo_hbm, wo, in_sem.at[1])
    resid_load = pltpu.make_async_copy(resid_hbm, raw.at[z], in_sem.at[2])
    weights = [
        pltpu.make_async_copy(src, dst, w_sem.at[i])
        for i, (src, dst) in enumerate(((wg_hbm, wg), (wu_hbm, wu), (wd_hbm, wd)))
    ]
    for copy in loads:
        copy.start()
    q_load.start()

    for p in range(pairs):
        for s in range(SPLITS):
            cols = slice(s * keys, (s + 1) * keys)
            doc_row = docs_ref[:, cols].astype(F32)
            aux_ref[p * SPLITS + s] = jnp.concatenate(
                [gates_ref[p * hpp : (p + 1) * hpp, cols]] + [doc_row] * (8 - hpp), axis=0
            )
    route_own[...] = jnp.concatenate([routes_ref[...]] * 4, axis=0)

    barrier = pltpu.get_barrier_semaphore()

    def greet(k, carry):
        pl.semaphore_signal(
            barrier,
            inc=1,
            device_id={"sp": lax.rem(me + k, n), "tp": t},
            device_id_type=MESH,
        )
        return carry

    lax.fori_loop(1, n, greet, 0)
    for other in (near_id, far_id, diag_id):
        pl.semaphore_signal(barrier, inc=1, device_id=other, device_id_type=MESH)

    def remote(src, dst, send, recv, to):
        return pltpu.make_async_remote_copy(
            src_ref=src, dst_ref=dst, send_sem=send, recv_sem=recv, device_id=to, device_id_type=MESH
        )

    def up(d, i):
        return remote(
            kv.at[d, i],
            kv.at[d + 1, i],
            up_send.at[d * chunks + i],
            up_recv.at[d * chunks + i],
            above_id,
        )

    def over(d, i):
        return remote(
            kv.at[d, i],
            kv.at[reach + 1 + d, i],
            over_send.at[d * chunks + i],
            over_recv.at[d * chunks + i],
            mate_id,
        )

    def aux_copy(k):
        return remote(
            aux_ref,
            aux_all.at[k],
            aux_send.at[k],
            aux_recv.at[k],
            {"sp": lax.rem(me + k, n), "tp": t},
        )

    def rising(d):
        return (z + 1 < floors) & (z >= d) & (d < reach)

    def crossing(d):
        return (z >= d) & ((d > 0) | (y == 0)) & ((d < reach) | (y == 1))

    def coming(d):
        return (z >= d) & ((d > 0) | (y == 1)) & ((d < reach) | (y == 0))

    def forward(d, i):
        @pl.when(rising(d))
        def _():
            up(d, i).start()

        @pl.when(crossing(d))
        def _():
            over(d, i).start()

    for copy in loads:
        copy.wait()
    pl.semaphore_wait(barrier, n + 2)
    lax.fori_loop(0, chunks, lambda i, z_: (forward(0, i), z_)[1], 0)

    def send_aux(k, carry):
        @pl.when(me + k < n)
        def _():
            aux_copy(k).start()

        return carry

    lax.fori_loop(1, n // 2 + 1, send_aux, 0)

    def route_copy(b):
        return remote(
            route_own,
            route_all.at[z],
            route_send.at[b],
            route_recv.at[z],
            {"sp": 2 * b + y, "tp": t},
        )

    def route_in(b):
        return remote(route_own, route_all.at[b], route_send.at[b], route_recv.at[b], near_id)

    def send_route(b, carry):
        @pl.when(b != z)
        def _():
            route_copy(b).start()

        return carry

    lax.fori_loop(0, floors, send_route, 0)
    wo_load.start()
    resid_load.start()
    for copy in weights:
        copy.start()

    lane = lax.broadcasted_iota(jnp.int32, (1, LANES), 1)
    tile = min(tokens, 256)

    def mine(h):
        return (lane >= h * head_size) & (lane < (h + 1) * head_size)

    q_load.wait()
    for p in range(pairs):
        block = q_in[:, p * LANES : (p + 1) * LANES].astype(F32) * (head_size ** (-0.5))
        for h in range(hpp):
            qs[p, h] = jnp.where(mine(h), block, 0.0).astype(BF)
    top[...] = jnp.full(top.shape, NEG, F32)
    acc[...] = jnp.zeros(acc.shape, F32)

    def wider(x):
        return jnp.concatenate([x] * (keys // LANES), axis=1) if keys > LANES else x[:, :keys]

    def visit(slot, i, p, h, r0, bias, allowed):
        at = pl.ds(r0, tile)
        k = kv[slot, i, 0]
        v = jnp.where(mine(h), kv[slot, i, 1].astype(F32), 1.0).astype(BF)
        scores = lax.dot_general(
            qs[p, h, at, :], k, (((1,), (1,)), ((), ())), preferred_element_type=F32
        )
        scores = scores + bias
        if allowed is not None:
            scores = jnp.where(allowed, scores, NEG)
        before = top[p, h, at, :]
        highest = jnp.maximum(before, jnp.max(scores, axis=1, keepdims=True))
        exps = jnp.exp(scores - wider(highest))
        rescale = jnp.exp(before - highest)
        top[p, h, at, :] = highest
        acc[p, h, at, :] = acc[p, h, at, :] * rescale + jnp.dot(
            exps.astype(BF), v, preferred_element_type=F32
        )

    first_doc = aux_ref[0][hpp : hpp + 1, 0:1]
    spots_r = lax.broadcasted_iota(jnp.int32, (keys, keys), 0)
    spots_c = lax.broadcasted_iota(jnp.int32, (keys, keys), 1)
    doc_cols = [
        jnp.sum(
            jnp.where(spots_r == spots_c, aux_ref[s][hpp : hpp + 1, :], 0.0), axis=1, keepdims=True
        )
        for s in range(SPLITS)
    ]
    doc_col = jnp.concatenate(doc_cols, axis=0)

    def diagonal(p, carry):
        for s in range(SPLITS):
            i = p * SPLITS + s
            side = aux_ref[i]
            for h in range(hpp):
                base = aux_ref[p * SPLITS][h : h + 1, 0:1]
                bias = base - side[h : h + 1, :]
                for r0 in range(0, tokens, tile):
                    if r0 + tile <= s * keys:
                        continue
                    key_pos = s * keys + lax.broadcasted_iota(jnp.int32, (1, keys), 1)
                    query_pos = r0 + lax.broadcasted_iota(jnp.int32, (tile, 1), 0)
                    allowed = (key_pos <= query_pos) & (
                        side[hpp : hpp + 1, :] == doc_col[r0 : r0 + tile]
                    )
                    visit(0, i, p, h, r0, bias, allowed)
        return carry

    lax.fori_loop(0, pairs, diagonal, 0)
    shut = jnp.where(doc_col == first_doc, 0.0, 2e30)
    for p in range(pairs):
        for h in range(hpp):
            top[p, h] = jnp.where(shut > 0.0, 1e30, top[p, h])

    def earlier(slot, dist, i):
        p = i // SPLITS
        side = aux_all[dist, i]
        zero = aux_ref[p * SPLITS]
        for h in range(hpp):
            bias = jnp.where(
                side[hpp : hpp + 1, :] == first_doc, zero[h : h + 1, 0:1] - side[h : h + 1, :], NEG
            )
            for r0 in range(0, tokens, tile):
                visit(slot, i, p, h, r0, bias, None)

    def aux_here(k, i):
        @pl.when(i == 0)
        def _():
            aux_copy(k).wait_recv()

    def crossed(d, i):
        @pl.when(coming(d))
        def _():
            dist = 2 * d + 2 * y - 1
            aux_here(dist, i)
            over(d, i).wait_recv()
            earlier(reach + 1 + d, dist, i)

    def history(j, carry):
        d, i = j // chunks + 1, lax.rem(j, chunks)

        @pl.when(z >= d)
        def _():
            up(d - 1, i).wait_recv()
            forward(d, i)
            aux_here(2 * d, i)
            earlier(d, 2 * d, i)

        @pl.when(d >= 2)
        def _():
            crossed(d - 2, i)

        return carry

    lax.fori_loop(0, reach * chunks, history, 0)
    lax.fori_loop(0, chunks, lambda i, z_: (crossed(reach - 1, i), z_)[1], 0)
    lax.fori_loop(0, chunks, lambda i, z_: (crossed(reach, i), z_)[1], 0)

    def h_copy(q, to):
        return remote(normed.at[q], gathered.at[t], h_send.at[q], h_recv.at[t], to)

    def h_in(q):
        return remote(normed.at[q], gathered.at[q], h_send.at[q], h_recv.at[q], near_id)

    def settle(q):
        at = pl.ds(pl.multiple_of(q * rows, rows), rows)
        for p in range(pairs):
            total = None
            for h in range(hpp):
                state = acc[p, h, at, :]
                sums = pltpu.roll(state, head_size, 1)
                attended = jnp.where(mine(h), state / sums, 0.0)
                mean_square = jnp.sum(attended * attended, axis=1, keepdims=True) / head_size
                piece = attended * lax.rsqrt(mean_square + EPS)
                total = piece if total is None else total + piece
            cols = slice(p * LANES, (p + 1) * LANES)
            normed[q, :, cols] = (total * gain_ref[:, cols]).astype(BF)

    for q, to in ((far, far_id), (diag, diag_id), (near, near_id)):
        settle(q)
        h_copy(q, to).start()
    settle(t)

    wide_tile = 512 if width % 512 == 0 else width
    row_r = lax.broadcasted_iota(jnp.int32, (rows, rows), 0)
    row_c = lax.broadcasted_iota(jnp.int32, (rows, rows), 1)

    def column(row):
        return jnp.sum(jnp.where(row_r == row_c, row, 0.0), axis=1, keepdims=True)

    before_row = (row_r < row_c).astype(F32).astype(BF)
    slots = lax.broadcasted_iota(jnp.int32, (cap, 1), 0).astype(F32)

    def taken(routes, e):
        named = ((routes[0:1, :] == e) | (routes[1:2, :] == e)).astype(F32)
        spread_out = jnp.broadcast_to(named, (8, rows)).astype(BF)
        rank = jnp.dot(spread_out, before_row, preferred_element_type=F32)[0:1]
        return ((named > 0.0) & (rank == slots)).astype(F32).astype(BF)

    first_e, second_e = [column(routes_ref[r : r + 1, :].astype(F32)) for r in range(2)]
    lane_f = lane.astype(F32)
    named = ((first_e == lane_f) | (second_e == lane_f)).astype(F32)
    ranks = jnp.dot(
        (row_c < row_r).astype(F32).astype(BF), named.astype(BF), preferred_element_type=F32
    )
    wants = []
    for e in (first_e, second_e):
        rank = jnp.sum(jnp.where(e == lane_f, ranks, 0.0), axis=1, keepdims=True)
        wants.append(e * cap + rank)
    wants = jnp.concatenate(wants, axis=0)
    route_weights = [column(route_w_ref[r : r + 1, :]) for r in range(2)]

    wo_load.wait()
    resid_load.wait()

    def product(src, q, at):
        return jnp.dot(
            src,
            wo[pl.ds(pl.multiple_of(q * width_here, width_here), width_here), at : at + wide_tile],
            preferred_element_type=F32,
        )

    for at in range(0, width, wide_tile):
        wide[:, at : at + wide_tile] = product(normed[t], t, at)
    h_in(near).wait_recv()
    for at in range(0, width, wide_tile):
        wide[:, at : at + wide_tile] += product(gathered[near], near, at)
    h_in(far).wait_recv()
    h_in(diag).wait_recv()
    squares = jnp.zeros((rows, 1), F32)
    for at in range(0, width, wide_tile):
        cols = slice(at, at + wide_tile)
        value = (
            wide[:, cols]
            + product(gathered[far], far, at)
            + product(gathered[diag], diag, at)
            + raw[z, :, cols].astype(F32)
        )
        value = value.astype(BF).astype(F32)
        wide[:, cols] = value
        squares = squares + jnp.sum(value * value, axis=1, keepdims=True)
    scale = lax.rsqrt(squares / width + EPS)
    halves = 2
    half = width // halves

    def raw_part(b, h):
        return raw.at[b, :, pl.ds(h * half, half)]

    def carry_raw(b, h, send, to):
        return remote(
            raw_part(b, h), raw_part(b, h), send.at[b * halves + h], raw_recv.at[b * halves + h], to
        )

    def rise(b, h):
        return carry_raw(b, h, rise_send, above_id)

    def fall(b, h):
        return carry_raw(b, h, fall_send, below_id)

    for h in range(halves):
        for at in range(h * half, (h + 1) * half, min(wide_tile, half)):
            cols = slice(at, at + min(wide_tile, half))
            raw[z, :, cols] = (wide[:, cols] * scale * norm_gain_ref[:, cols]).astype(BF)

        @pl.when(z + 1 < floors)
        def _():
            rise(z, h).start()

        @pl.when(z > 0)
        def _():
            fall(z, h).start()

    def floor_at(j):
        return jnp.where(j <= z, z - j, j)

    def source(k):
        return 2 * floor_at(k // 2) + jnp.where(lax.rem(k, 2) == 0, y, 1 - y)

    def arrive(j):
        below, above = z - j, z + j

        @pl.when(below >= 0)
        def _():
            for h in range(halves):
                rise(below, h).wait_recv()

                @pl.when(z + 1 < floors)
                def _():
                    rise(below, h).start()

        @pl.when(above < floors)
        def _():
            for h in range(halves):
                fall(above, h).wait_recv()

                @pl.when(z > 0)
                def _():
                    fall(above, h).start()

    def y_copy(b):
        return remote(
            crossing_rows.at[b], fan.at[2 * b + y, t], y_send.at[b], y_recv.at[b], mate_id
        )

    def y_in(b):
        return remote(
            crossing_rows.at[b], fan.at[2 * b + 1 - y, t], y_send.at[b], y_recv.at[b], mate_id
        )

    def select(b, routes):
        mate = me + 1 - 2 * y
        picks = jnp.concatenate([taken(routes, mate), taken(routes, me)], axis=0)
        for at in range(0, width, wide_tile):
            cols = slice(at, at + wide_tile)
            both = jnp.dot(picks, raw[b, :, cols], preferred_element_type=F32).astype(BF)
            crossing_rows[b, :, cols] = both[:cap]
            fan[2 * b + y, t, :, cols] = both[cap:]
        y_copy(b).start()

    def x_copy(k, q):
        p = source(k)
        return remote(fan.at[p, q], fan.at[p, q], x_send.at[p], x_recv.at[p], far_id)

    def c_copy(k, q):
        p = source(k)
        return remote(fan.at[p, q], fan.at[p, q], c_send.at[p], c_recv.at[p], near_id)

    def d_copy(k, q):
        p = source(k)
        return remote(fan.at[p, q], fan.at[p, q], d_send.at[p], d_recv.at[p], near_id)

    def p_copy(k):
        p = source(k)
        return remote(part.at[p, 1 - c], got.at[p], p_send.at[p], p_recv.at[p], near_id)

    def s_copy(k):
        p = source(k)
        return remote(part.at[p, c, 1 - xi], across.at[p], s_send.at[p], s_recv.at[p], far_id)

    def r_out(k):
        p = source(k)
        return remote(
            part.at[p, c, xi], ret_ref.at[me], r_send.at[p], r_recv.at[me], {"sp": p, "tp": t}
        )

    def r_in(p):
        return remote(part.at[p, c, xi], ret_ref.at[p], r_send.at[p], r_recv.at[p], near_id)

    def spread(k):
        x_copy(k, t).start()
        c_copy(k, t).start()

    def step_a(k):
        j = k // 2

        @pl.when(lax.rem(k, 2) == 0)
        def _():
            arrive(j)
            route_in(floor_at(j)).wait_recv()
            select(floor_at(j), route_all[floor_at(j)])

        @pl.when(lax.rem(k, 2) == 1)
        def _():
            y_in(floor_at(j)).wait_recv()

        spread(k)

    def step_x(k):
        x_copy(k, far).wait_recv()
        d_copy(k, far).start()

    def step_compute(k):
        p = source(k)
        c_copy(k, near).wait_recv()
        d_copy(k, diag).wait_recv()
        block = fan[p].reshape(4 * cap, width)
        gate = jnp.dot(block, wg[...], preferred_element_type=F32)
        up_ = jnp.dot(block, wu[...], preferred_element_type=F32)
        hidden[...] = (gate * jax.nn.sigmoid(gate) * up_).astype(BF)
        for at in range(0, width, wide_tile):
            down = jnp.dot(
                hidden[...], wd[:, at : at + wide_tile], preferred_element_type=F32
            ).astype(BF)
            for q in range(4):
                part[p, q % 2, q // 2, :, at : at + wide_tile] = down[q * cap : (q + 1) * cap]
        p_copy(k).start()

    def step_pair(k):
        p = source(k)
        p_copy(k).wait_recv()
        part[p, c, 1 - xi] = (
            part[p, c, 1 - xi].astype(F32) + got[p, 1 - xi].astype(F32)
        ).astype(BF)
        s_copy(k).start()

    def step_final(k):
        p = source(k)
        s_copy(k).wait_recv()
        total = (
            part[p, c, xi].astype(F32) + got[p, xi].astype(F32) + across[p].astype(F32)
        ).astype(BF)

        @pl.when(k == 0)
        def _():
            ret_ref[me] = total

        @pl.when(k > 0)
        def _():
            part[p, c, xi] = total
            r_out(k).start()

    select(z, routes_ref[...])
    spread(0)
    step_a(1)
    step_x(0)
    for copy in weights:
        copy.wait()

    def iteration(i, carry):
        @pl.when(i + 2 < n)
        def _():
            step_a(i + 2)

        @pl.when(i + 1 < n)
        def _():
            step_x(i + 1)

        @pl.when((i >= 1) & (i < n + 1))
        def _():
            step_pair(i - 1)

        @pl.when(i < n)
        def _():
            step_compute(i)

        @pl.when(i >= 2)
        def _():
            step_final(i - 2)

        return carry

    lax.fori_loop(0, n + 2, iteration, 0)

    slot = lax.broadcasted_iota(jnp.int32, (1, cap), 1)

    def combine(p):
        picks = (wants == (p * cap + slot).astype(F32)).astype(F32).astype(BF)
        for at in range(0, width, wide_tile):
            cols = slice(at, at + wide_tile)
            chosen = jnp.dot(picks, ret_ref[p, :, cols], preferred_element_type=F32)
            wide[:, cols] += (
                route_weights[0] * chosen[:rows] + route_weights[1] * chosen[rows:]
            )

    combine(me)

    def gather(i, carry):
        p = source(i)
        r_in(p).wait_recv()
        combine(p)
        return carry

    lax.fori_loop(1, n, gather, 0)
    mixed_ref[...] = wide[...].astype(BF)

    def sent_history(j, carry):
        d, i = j // chunks, lax.rem(j, chunks)

        @pl.when(rising(d))
        def _():
            up(d, i).wait_send()

        @pl.when(crossing(d))
        def _():
            over(d, i).wait_send()

        return carry

    lax.fori_loop(0, (reach + 1) * chunks, sent_history, 0)

    def sent_aux(k, carry):
        @pl.when(me + k < n)
        def _():
            aux_copy(k).wait_send()

        return carry

    lax.fori_loop(1, n // 2 + 1, sent_aux, 0)
    for q, to in ((far, far_id), (diag, diag_id), (near, near_id)):
        h_copy(q, to).wait_send()

    def sent_floor(b, carry):
        y_copy(b).wait_send()

        @pl.when(b != z)
        def _():
            route_copy(b).wait_send()

        for h in range(halves):
            @pl.when((b <= z) & (z + 1 < floors))
            def _():
                rise(b, h).wait_send()

            @pl.when((b >= z) & (z > 0))
            def _():
                fall(b, h).wait_send()

        return carry

    lax.fori_loop(0, floors, sent_floor, 0)

    def finish(k, carry):
        x_copy(k, t).wait_send()
        c_copy(k, t).wait_send()
        d_copy(k, far).wait_send()
        p_copy(k).wait_send()
        s_copy(k).wait_send()

        @pl.when(k > 0)
        def _():
            r_out(k).wait_send()

        return carry

    lax.fori_loop(0, n, finish, 0)


def on_device(
    queries,
    keys,
    values,
    cum_gate,
    documents,
    head_gain,
    out_weight,
    resid,
    norm_gain,
    routes,
    route_weights,
    w_gate,
    w_up,
    w_down,
):
    tokens, width_here = queries.shape
    heads_here = cum_gate.shape[1]
    head_size = width_here // heads_here
    n = lax.axis_size("sp")
    tp_count = lax.axis_size("tp")
    rows, width = resid.shape
    top_count = routes.shape[1]
    cap = 2 * top_count * tokens // (tp_count * n)
    hid = w_gate.shape[2]
    pairs, hpp = width_here // LANES, LANES // head_size
    part_len = tokens // SPLITS
    chunks = pairs * SPLITS
    reach = n // 4

    dma = pltpu.SemaphoreType.DMA
    hbm = pl.BlockSpec(memory_space=pl.ANY)
    vmem = pl.BlockSpec(memory_space=pltpu.VMEM)
    return pl.pallas_call(
        functools.partial(layer_kernel, n, head_size, cap),
        out_shape=jax.ShapeDtypeStruct((rows, width), BF),
        in_specs=[hbm] * 3 + [vmem] * 3 + [hbm] * 2 + [vmem] * 3 + [hbm] * 3,
        out_specs=vmem,
        scratch_shapes=[
            pltpu.VMEM((tokens, width_here), BF),
            pltpu.VMEM((pairs, hpp, tokens, LANES), BF),
            pltpu.VMEM((2 * reach + 2, chunks, 2, part_len, LANES), BF),
            pltpu.VMEM((chunks, 8, part_len), F32),
            pltpu.VMEM((n // 2 + 1, chunks, 8, part_len), F32),
            pltpu.VMEM((8, rows), jnp.int32),
            pltpu.VMEM((n // 2, 8, rows), jnp.int32),
            pltpu.VMEM((pairs, hpp, tokens, LANES), F32),
            pltpu.VMEM((pairs, hpp, tokens, LANES), F32),
            pltpu.VMEM((tp_count, rows, width_here), BF),
            pltpu.VMEM((tp_count, rows, width_here), BF),
            pltpu.VMEM((tp_count * width_here, width), BF),
            pltpu.VMEM((rows, width), F32),
            pltpu.VMEM((n // 2, rows, width), BF),
            pltpu.VMEM((n // 2, cap, width), BF),
            pltpu.VMEM((n, cap, width), BF),
            pltpu.VMEM((n, 4, cap, width), BF),
            pltpu.VMEM((width, hid), BF),
            pltpu.VMEM((width, hid), BF),
            pltpu.VMEM((hid, width), BF),
            pltpu.VMEM((4 * cap, hid), BF),
            pltpu.VMEM((n, 2, 2, cap, width), BF),
            pltpu.VMEM((n, 2, cap, width), BF),
            pltpu.VMEM((n, cap, width), BF),
            dma((3,)),
            dma((2 * chunks,)),
            dma((3,)),
        ]
        + [dma(((reach + 1) * chunks,)) for _ in range(4)]
        + [dma((n // 2 + 1,)) for _ in range(2)]
        + [dma((tp_count,)) for _ in range(2)]
        + [dma((n // 2,)) for _ in range(2)]
        + [dma((n,)) for _ in range(3)]
        + [dma((n // 2,)) for _ in range(2)]
        + [dma((n,)) for _ in range(12)],
        compiler_params=pltpu.CompilerParams(
            collective_id=1, has_side_effects=True, vmem_limit_bytes=VMEM_LIMIT
        ),
    )(
        queries,
        keys,
        values,
        cum_gate.T,
        documents[None, :],
        head_gain[None, :],
        out_weight,
        resid,
        norm_gain[None, :],
        routes.T,
        route_weights.T,
        w_gate[0],
        w_up[0],
        w_down[0],
    )


def solution(mesh):
    in_specs = (
        P("sp", "tp"),
        P("sp", "tp"),
        P("sp", "tp"),
        P("sp", "tp"),
        P("sp"),
        P("tp"),
        P(),
        P(("sp", "tp"), None),
        P(),
        P(("sp", "tp"), None),
        P(("sp", "tp"), None),
        P("sp", None, "tp"),
        P("sp", None, "tp"),
        P("sp", "tp", None),
    )
    out_specs = P(("sp", "tp"), None)
    return jax.shard_map(
        on_device, mesh=mesh, in_specs=in_specs, out_specs=out_specs, check_vma=False
    )
```

```python
import functools

import jax
import jax.numpy as jnp
from jax import lax
from jax.experimental import pallas as pl
from jax.experimental.pallas import tpu as pltpu
from jax.sharding import PartitionSpec as P

EPS = 1e-06
MESH = pl.DeviceIdType.MESH
NEG = -1e30
VMEM_LIMIT = 67043328
LANES = 128
SPLITS = 2
BF = jnp.bfloat16
F32 = jnp.float32


def layer_kernel(
    n,
    head_size,
    cap,
    q_hbm,
    k_hbm,
    v_hbm,
    gates_ref,
    docs_ref,
    gain_ref,
    wo_hbm,
    resid_hbm,
    norm_gain_ref,
    routes_ref,
    route_w_ref,
    wg_hbm,
    wu_hbm,
    wd_hbm,
    mixed_ref,
    q_in,
    qs,
    kv,
    aux_ref,
    aux_all,
    route_own,
    route_all,
    top,
    acc,
    normed,
    gathered,
    wo,
    wide,
    raw,
    crossing_rows,
    ret_ref,
    fan,
    wg,
    wu,
    wd,
    hidden,
    part,
    got,
    across,
    in_sem,
    kv_sem,
    w_sem,
    up_send,
    up_recv,
    over_send,
    over_recv,
    aux_send,
    aux_recv,
    h_send,
    h_recv,
    route_send,
    route_recv,
    rise_send,
    fall_send,
    raw_recv,
    y_send,
    y_recv,
    x_send,
    x_recv,
    c_send,
    c_recv,
    d_send,
    d_recv,
    p_send,
    p_recv,
    s_send,
    s_recv,
    r_send,
    r_recv,
):
    me = lax.axis_index("sp")
    t = lax.axis_index("tp")
    c, xi = lax.rem(t, 2), t // 2
    near = xi * 2 + (1 - c)
    far = (1 - xi) * 2 + c
    diag = 3 - t
    y, z = lax.rem(me, 2), me // 2
    floors, reach = n // 2, n // 4
    near_id = {"sp": me, "tp": near}
    far_id = {"sp": me, "tp": far}
    diag_id = {"sp": me, "tp": diag}
    mate_id = {"sp": me + 1 - 2 * y, "tp": t}
    above_id = {"sp": lax.rem(me + 2, n), "tp": t}
    below_id = {"sp": lax.rem(me + n - 2, n), "tp": t}

    tokens, width_here = q_in.shape
    pairs = width_here // LANES
    hpp = LANES // head_size
    keys = tokens // SPLITS
    chunks = pairs * SPLITS
    rows, width = mixed_ref.shape

    loads = [
        pltpu.make_async_copy(
            src.at[pl.ds(s * keys, keys), pl.ds(p * LANES, LANES)],
            kv.at[0, p * SPLITS + s, j],
            kv_sem.at[(p * SPLITS + s) * 2 + j],
        )
        for p in range(pairs)
        for s in range(SPLITS)
        for j, src in enumerate((k_hbm, v_hbm))
    ]
    q_load = pltpu.make_async_copy(q_hbm, q_in, in_sem.at[0])
    wo_load = pltpu.make_async_copy(wo_hbm, wo, in_sem.at[1])
    resid_load = pltpu.make_async_copy(resid_hbm, raw.at[z], in_sem.at[2])
    weights = [
        pltpu.make_async_copy(src, dst, w_sem.at[i])
        for i, (src, dst) in enumerate(((wg_hbm, wg), (wu_hbm, wu), (wd_hbm, wd)))
    ]
    for copy in loads:
        copy.start()
    q_load.start()

    heads = pairs * hpp
    for s in range(SPLITS):
        cols = slice(s * keys, (s + 1) * keys)
        doc_row = docs_ref[:, cols].astype(F32)
        aux_ref[s] = jnp.concatenate(
            [gates_ref[:, cols]] + [doc_row] * (aux_ref.shape[1] - heads), axis=0
        )
    route_own[...] = jnp.concatenate([routes_ref[...]] * 4, axis=0)

    barrier = pltpu.get_barrier_semaphore()

    def greet(k, carry):
        pl.semaphore_signal(
            barrier,
            inc=1,
            device_id={"sp": lax.rem(me + k, n), "tp": t},
            device_id_type=MESH,
        )
        return carry

    lax.fori_loop(1, n, greet, 0)
    for other in (near_id, far_id, diag_id):
        pl.semaphore_signal(barrier, inc=1, device_id=other, device_id_type=MESH)

    def remote(src, dst, send, recv, to):
        return pltpu.make_async_remote_copy(
            src_ref=src, dst_ref=dst, send_sem=send, recv_sem=recv, device_id=to, device_id_type=MESH
        )

    def up(d, i):
        return remote(
            kv.at[d, i],
            kv.at[d + 1, i],
            up_send.at[d * chunks + i],
            up_recv.at[d * chunks + i],
            above_id,
        )

    def over(d, i):
        return remote(
            kv.at[d, i],
            kv.at[reach + 1 + d, i],
            over_send.at[d * chunks + i],
            over_recv.at[d * chunks + i],
            mate_id,
        )

    def aux_copy(k):
        return remote(
            aux_ref,
            aux_all.at[k],
            aux_send.at[k],
            aux_recv.at[k],
            {"sp": lax.rem(me + k, n), "tp": t},
        )

    def rising(d):
        return (z + 1 < floors) & (z >= d) & (d < reach)

    def crossing(d):
        return (z >= d) & ((d > 0) | (y == 0)) & ((d < reach) | (y == 1))

    def coming(d):
        return (z >= d) & ((d > 0) | (y == 1)) & ((d < reach) | (y == 0))

    def forward(d, i):
        @pl.when(rising(d))
        def _():
            up(d, i).start()

        @pl.when(crossing(d))
        def _():
            over(d, i).start()

    pl.semaphore_wait(barrier, n + 2)

    def send_aux(k, carry):
        @pl.when(me + k < n)
        def _():
            aux_copy(k).start()

        return carry

    lax.fori_loop(1, n // 2 + 1, send_aux, 0)
    for copy in loads:
        copy.wait()
    lax.fori_loop(0, chunks, lambda i, z_: (forward(0, i), z_)[1], 0)

    def route_copy(b):
        return remote(
            route_own,
            route_all.at[z],
            route_send.at[b],
            route_recv.at[z],
            {"sp": 2 * b + y, "tp": t},
        )

    def route_in(b):
        return remote(route_own, route_all.at[b], route_send.at[b], route_recv.at[b], near_id)

    def send_route(b, carry):
        @pl.when(b != z)
        def _():
            route_copy(b).start()

        return carry

    lax.fori_loop(0, floors, send_route, 0)
    wo_load.start()
    resid_load.start()
    for copy in weights:
        copy.start()

    lane = lax.broadcasted_iota(jnp.int32, (1, LANES), 1)
    tile = min(tokens, 256)

    def mine(h):
        return (lane >= h * head_size) & (lane < (h + 1) * head_size)

    q_load.wait()
    for p in range(pairs):
        block = q_in[:, p * LANES : (p + 1) * LANES].astype(F32) * (head_size ** (-0.5))
        for h in range(hpp):
            qs[p, h] = jnp.where(mine(h), block, 0.0).astype(BF)
    top[...] = jnp.full(top.shape, NEG, F32)
    acc[...] = jnp.zeros(acc.shape, F32)

    def wider(x):
        return jnp.concatenate([x] * (keys // LANES), axis=1) if keys > LANES else x[:, :keys]

    def visit(slot, i, p, h, r0, bias, allowed):
        at = pl.ds(r0, tile)
        k = kv[slot, i, 0]
        v = jnp.where(mine(h), kv[slot, i, 1].astype(F32), 1.0).astype(BF)
        scores = lax.dot_general(
            qs[p, h, at, :], k, (((1,), (1,)), ((), ())), preferred_element_type=F32
        )
        scores = scores + bias
        if allowed is not None:
            scores = jnp.where(allowed, scores, NEG)
        before = top[p, h, at, :]
        highest = jnp.maximum(before, jnp.max(scores, axis=1, keepdims=True))
        exps = jnp.exp(scores - wider(highest))
        rescale = jnp.exp(before - highest)
        top[p, h, at, :] = highest
        acc[p, h, at, :] = acc[p, h, at, :] * rescale + jnp.dot(
            exps.astype(BF), v, preferred_element_type=F32
        )

    first_doc = aux_ref[0, heads : heads + 1, 0:1]
    spots_r = lax.broadcasted_iota(jnp.int32, (keys, keys), 0)
    spots_c = lax.broadcasted_iota(jnp.int32, (keys, keys), 1)
    doc_cols = [
        jnp.sum(
            jnp.where(spots_r == spots_c, aux_ref[s, heads : heads + 1, :], 0.0), axis=1, keepdims=True
        )
        for s in range(SPLITS)
    ]
    doc_col = jnp.concatenate(doc_cols, axis=0)

    def diagonal(p, carry):
        for s in range(SPLITS):
            i = p * SPLITS + s
            docs_here = aux_ref[s, heads : heads + 1, :]
            for h in range(hpp):
                gate_at = pl.ds(p * hpp + h, 1)
                bias = aux_ref[0, gate_at, :][:, 0:1] - aux_ref[s, gate_at, :]
                for r0 in range(0, tokens, tile):
                    if r0 + tile <= s * keys:
                        continue
                    key_pos = s * keys + lax.broadcasted_iota(jnp.int32, (1, keys), 1)
                    query_pos = r0 + lax.broadcasted_iota(jnp.int32, (tile, 1), 0)
                    allowed = (key_pos <= query_pos) & (
                        docs_here == doc_col[r0 : r0 + tile]
                    )
                    visit(0, i, p, h, r0, bias, allowed)
        return carry

    lax.fori_loop(0, pairs, diagonal, 0)
    shut = jnp.where(doc_col == first_doc, 0.0, 2e30)
    for p in range(pairs):
        for h in range(hpp):
            top[p, h] = jnp.where(shut > 0.0, 1e30, top[p, h])

    def earlier(slot, dist, i):
        p, s = i // SPLITS, lax.rem(i, SPLITS)
        same = aux_all[dist, s, heads : heads + 1, :] == first_doc
        for h in range(hpp):
            gate_at = pl.ds(p * hpp + h, 1)
            bias = jnp.where(
                same, aux_ref[0, gate_at, :][:, 0:1] - aux_all[dist, s, gate_at, :], NEG
            )
            for r0 in range(0, tokens, tile):
                visit(slot, i, p, h, r0, bias, None)

    def aux_here(k, i):
        @pl.when(i == 0)
        def _():
            aux_copy(k).wait_recv()

    def crossed(d, i):
        @pl.when(coming(d))
        def _():
            dist = 2 * d + 2 * y - 1
            aux_here(dist, i)
            over(d, i).wait_recv()
            earlier(reach + 1 + d, dist, i)

    def history(j, carry):
        d, i = j // chunks + 1, lax.rem(j, chunks)

        @pl.when(z >= d)
        def _():
            up(d - 1, i).wait_recv()
            forward(d, i)
            aux_here(2 * d, i)
            earlier(d, 2 * d, i)

        @pl.when(d >= 2)
        def _():
            crossed(d - 2, i)

        return carry

    lax.fori_loop(0, reach * chunks, history, 0)
    lax.fori_loop(0, chunks, lambda i, z_: (crossed(reach - 1, i), z_)[1], 0)
    lax.fori_loop(0, chunks, lambda i, z_: (crossed(reach, i), z_)[1], 0)

    def h_copy(q, to):
        return remote(normed.at[q], gathered.at[t], h_send.at[q], h_recv.at[t], to)

    def h_in(q):
        return remote(normed.at[q], gathered.at[q], h_send.at[q], h_recv.at[q], near_id)

    def settle(q):
        at = pl.ds(pl.multiple_of(q * rows, rows), rows)
        for p in range(pairs):
            total = None
            for h in range(hpp):
                state = acc[p, h, at, :]
                sums = pltpu.roll(state, head_size, 1)
                attended = jnp.where(mine(h), state / sums, 0.0)
                mean_square = jnp.sum(attended * attended, axis=1, keepdims=True) / head_size
                piece = attended * lax.rsqrt(mean_square + EPS)
                total = piece if total is None else total + piece
            cols = slice(p * LANES, (p + 1) * LANES)
            normed[q, :, cols] = (total * gain_ref[:, cols]).astype(BF)

    for q, to in ((far, far_id), (diag, diag_id), (near, near_id)):
        settle(q)
        h_copy(q, to).start()
    settle(t)

    wide_tile = 512 if width % 512 == 0 else width
    row_r = lax.broadcasted_iota(jnp.int32, (rows, rows), 0)
    row_c = lax.broadcasted_iota(jnp.int32, (rows, rows), 1)

    def column(row):
        return jnp.sum(jnp.where(row_r == row_c, row, 0.0), axis=1, keepdims=True)

    before_row = (row_r < row_c).astype(F32).astype(BF)
    slots = lax.broadcasted_iota(jnp.int32, (cap, 1), 0).astype(F32)

    def taken(routes, e):
        named = ((routes[0:1, :] == e) | (routes[1:2, :] == e)).astype(F32)
        spread_out = jnp.broadcast_to(named, (8, rows)).astype(BF)
        rank = jnp.dot(spread_out, before_row, preferred_element_type=F32)[0:1]
        return ((named > 0.0) & (rank == slots)).astype(F32).astype(BF)

    first_e, second_e = [column(routes_ref[r : r + 1, :].astype(F32)) for r in range(2)]
    lane_f = lane.astype(F32)
    named = ((first_e == lane_f) | (second_e == lane_f)).astype(F32)
    ranks = jnp.dot(
        (row_c < row_r).astype(F32).astype(BF), named.astype(BF), preferred_element_type=F32
    )
    wants = []
    for e in (first_e, second_e):
        rank = jnp.sum(jnp.where(e == lane_f, ranks, 0.0), axis=1, keepdims=True)
        wants.append(e * cap + rank)
    wants = jnp.concatenate(wants, axis=0)
    route_weights = [column(route_w_ref[r : r + 1, :]) for r in range(2)]

    wo_load.wait()
    resid_load.wait()

    def product(src, q, at):
        return jnp.dot(
            src,
            wo[pl.ds(pl.multiple_of(q * width_here, width_here), width_here), at : at + wide_tile],
            preferred_element_type=F32,
        )

    for at in range(0, width, wide_tile):
        wide[:, at : at + wide_tile] = product(normed[t], t, at)
    h_in(near).wait_recv()
    for at in range(0, width, wide_tile):
        wide[:, at : at + wide_tile] += product(gathered[near], near, at)
    h_in(far).wait_recv()
    h_in(diag).wait_recv()
    squares = jnp.zeros((rows, 1), F32)
    for at in range(0, width, wide_tile):
        cols = slice(at, at + wide_tile)
        value = (
            wide[:, cols]
            + product(gathered[far], far, at)
            + product(gathered[diag], diag, at)
            + raw[z, :, cols].astype(F32)
        )
        value = value.astype(BF).astype(F32)
        wide[:, cols] = value
        squares = squares + jnp.sum(value * value, axis=1, keepdims=True)
    scale = lax.rsqrt(squares / width + EPS)
    halves = 2
    half = width // halves

    def raw_part(b, h):
        return raw.at[b, :, pl.ds(h * half, half)]

    def carry_raw(b, h, send, to):
        return remote(
            raw_part(b, h), raw_part(b, h), send.at[b * halves + h], raw_recv.at[b * halves + h], to
        )

    def rise(b, h):
        return carry_raw(b, h, rise_send, above_id)

    def fall(b, h):
        return carry_raw(b, h, fall_send, below_id)

    for h in range(halves):
        for at in range(h * half, (h + 1) * half, min(wide_tile, half)):
            cols = slice(at, at + min(wide_tile, half))
            raw[z, :, cols] = (wide[:, cols] * scale * norm_gain_ref[:, cols]).astype(BF)

        @pl.when(z + 1 < floors)
        def _():
            rise(z, h).start()

        @pl.when(z > 0)
        def _():
            fall(z, h).start()

    both_ways = jnp.minimum(z, floors - 1 - z)

    def floor_at(j):
        step = jnp.where(j <= 2 * both_ways, (j + 1) // 2, j - both_ways)
        down = jnp.where(j <= 2 * both_ways, lax.rem(j, 2) == 1, 2 * z >= floors)
        return jnp.where(down, z - step, z + step)

    def source(k):
        return 2 * floor_at(k // 2) + jnp.where(lax.rem(k, 2) == 0, y, 1 - y)

    def arrive(j):
        later = jnp.where(z > 0, j - 1, j)
        below, above = z - j, z + later

        @pl.when(below >= 0)
        def _():
            for h in range(halves):
                rise(below, h).wait_recv()

                @pl.when(z + 1 < floors)
                def _():
                    rise(below, h).start()

        @pl.when((above < floors) & (later > 0))
        def _():
            for h in range(halves):
                fall(above, h).wait_recv()

                @pl.when(z > 0)
                def _():
                    fall(above, h).start()

    def y_copy(b):
        return remote(
            crossing_rows.at[b], fan.at[2 * b + y, t], y_send.at[b], y_recv.at[b], mate_id
        )

    def y_in(b):
        return remote(
            crossing_rows.at[b], fan.at[2 * b + 1 - y, t], y_send.at[b], y_recv.at[b], mate_id
        )

    def select(b, routes):
        mate = me + 1 - 2 * y
        picks = jnp.concatenate([taken(routes, mate), taken(routes, me)], axis=0)
        for at in range(0, width, wide_tile):
            cols = slice(at, at + wide_tile)
            both = jnp.dot(picks, raw[b, :, cols], preferred_element_type=F32).astype(BF)
            crossing_rows[b, :, cols] = both[:cap]
            fan[2 * b + y, t, :, cols] = both[cap:]
        y_copy(b).start()

    def x_copy(k, q):
        p = source(k)
        return remote(fan.at[p, q], fan.at[p, q], x_send.at[p], x_recv.at[p], far_id)

    def c_copy(k, q):
        p = source(k)
        return remote(fan.at[p, q], fan.at[p, q], c_send.at[p], c_recv.at[p], near_id)

    def d_copy(k, q):
        p = source(k)
        return remote(fan.at[p, q], fan.at[p, q], d_send.at[p], d_recv.at[p], near_id)

    def p_copy(k):
        p = source(k)
        return remote(part.at[p, 1 - c], got.at[p], p_send.at[p], p_recv.at[p], near_id)

    def s_copy(k):
        p = source(k)
        return remote(part.at[p, c, 1 - xi], across.at[p], s_send.at[p], s_recv.at[p], far_id)

    def r_out(k):
        p = source(k)
        return remote(
            part.at[p, c, xi], ret_ref.at[me], r_send.at[p], r_recv.at[me], {"sp": p, "tp": t}
        )

    def r_in(p):
        return remote(part.at[p, c, xi], ret_ref.at[p], r_send.at[p], r_recv.at[p], near_id)

    def spread(k):
        x_copy(k, t).start()
        c_copy(k, t).start()

    def step_a(k):
        j = k // 2

        @pl.when(lax.rem(k, 2) == 0)
        def _():
            arrive(j)
            route_in(floor_at(j)).wait_recv()
            select(floor_at(j), route_all[floor_at(j)])

        @pl.when(lax.rem(k, 2) == 1)
        def _():
            y_in(floor_at(j)).wait_recv()

        spread(k)

    def step_x(k):
        x_copy(k, far).wait_recv()
        d_copy(k, far).start()

    def step_compute(k):
        p = source(k)
        c_copy(k, near).wait_recv()
        d_copy(k, diag).wait_recv()
        block = fan[p].reshape(4 * cap, width)
        gate = jnp.dot(block, wg[...], preferred_element_type=F32)
        up_ = jnp.dot(block, wu[...], preferred_element_type=F32)
        hidden[...] = (gate * jax.nn.sigmoid(gate) * up_).astype(BF)
        for at in range(0, width, wide_tile):
            down = jnp.dot(
                hidden[...], wd[:, at : at + wide_tile], preferred_element_type=F32
            ).astype(BF)
            for q in range(4):
                part[p, q % 2, q // 2, :, at : at + wide_tile] = down[q * cap : (q + 1) * cap]
        p_copy(k).start()

    def step_pair(k):
        p = source(k)
        p_copy(k).wait_recv()
        part[p, c, 1 - xi] = (
            part[p, c, 1 - xi].astype(F32) + got[p, 1 - xi].astype(F32)
        ).astype(BF)
        s_copy(k).start()

    def step_final(k):
        p = source(k)
        s_copy(k).wait_recv()
        total = (
            part[p, c, xi].astype(F32) + got[p, xi].astype(F32) + across[p].astype(F32)
        ).astype(BF)

        @pl.when(k == 0)
        def _():
            ret_ref[me] = total

        @pl.when(k > 0)
        def _():
            part[p, c, xi] = total
            r_out(k).start()

    select(z, routes_ref[...])
    spread(0)
    step_a(1)
    for k in (2, 3):
        step_a(k)
    for copy in weights:
        copy.wait()

    def turn(i):
        return jnp.where(i + 2 < n, i + 2, n - 1 - i)

    step_x(turn(0))

    def iteration(i, carry):
        @pl.when(i + 4 < n)
        def _():
            step_a(i + 4)

        @pl.when(i + 1 < n)
        def _():
            step_x(turn(i + 1))

        @pl.when(i >= 1)
        def _():
            step_pair(turn(i - 1))

        @pl.when(i < n)
        def _():
            step_compute(turn(i))

        @pl.when(i >= 2)
        def _():
            step_final(turn(i - 2))

        return carry

    lax.fori_loop(0, n + 1, iteration, 0)

    slot = lax.broadcasted_iota(jnp.int32, (1, cap), 1)

    def combine(p):
        picks = (wants == (p * cap + slot).astype(F32)).astype(F32).astype(BF)
        for at in range(0, width, wide_tile):
            cols = slice(at, at + wide_tile)
            chosen = jnp.dot(picks, ret_ref[p, :, cols], preferred_element_type=F32)
            wide[:, cols] += (
                route_weights[0] * chosen[:rows] + route_weights[1] * chosen[rows:]
            )

    def gather(i, carry):
        p = source(turn(i))
        r_in(p).wait_recv()
        combine(p)
        return carry

    lax.fori_loop(0, n - 2, gather, 0)
    step_final(0)
    combine(me)
    gather(n - 2, 0)
    mixed_ref[...] = wide[...].astype(BF)

    def sent_history(j, carry):
        d, i = j // chunks, lax.rem(j, chunks)

        @pl.when(rising(d))
        def _():
            up(d, i).wait_send()

        @pl.when(crossing(d))
        def _():
            over(d, i).wait_send()

        return carry

    lax.fori_loop(0, (reach + 1) * chunks, sent_history, 0)

    def sent_aux(k, carry):
        @pl.when(me + k < n)
        def _():
            aux_copy(k).wait_send()

        return carry

    lax.fori_loop(1, n // 2 + 1, sent_aux, 0)
    for q, to in ((far, far_id), (diag, diag_id), (near, near_id)):
        h_copy(q, to).wait_send()

    def sent_floor(b, carry):
        y_copy(b).wait_send()

        @pl.when(b != z)
        def _():
            route_copy(b).wait_send()

        for h in range(halves):
            @pl.when((b <= z) & (z + 1 < floors))
            def _():
                rise(b, h).wait_send()

            @pl.when((b >= z) & (z > 0))
            def _():
                fall(b, h).wait_send()

        return carry

    lax.fori_loop(0, floors, sent_floor, 0)

    def finish(k, carry):
        x_copy(k, t).wait_send()
        c_copy(k, t).wait_send()
        d_copy(k, far).wait_send()
        p_copy(k).wait_send()
        s_copy(k).wait_send()

        @pl.when(k > 0)
        def _():
            r_out(k).wait_send()

        return carry

    lax.fori_loop(0, n, finish, 0)


def on_device(
    queries,
    keys,
    values,
    cum_gate,
    documents,
    head_gain,
    out_weight,
    resid,
    norm_gain,
    routes,
    route_weights,
    w_gate,
    w_up,
    w_down,
):
    tokens, width_here = queries.shape
    heads_here = cum_gate.shape[1]
    head_size = width_here // heads_here
    n = lax.axis_size("sp")
    tp_count = lax.axis_size("tp")
    rows, width = resid.shape
    top_count = routes.shape[1]
    cap = 2 * top_count * tokens // (tp_count * n)
    hid = w_gate.shape[2]
    pairs, hpp = width_here // LANES, LANES // head_size
    part_len = tokens // SPLITS
    chunks = pairs * SPLITS
    reach = n // 4
    side_rows = -(-(heads_here + 1) // 8) * 8

    dma = pltpu.SemaphoreType.DMA
    hbm = pl.BlockSpec(memory_space=pl.ANY)
    vmem = pl.BlockSpec(memory_space=pltpu.VMEM)
    return pl.pallas_call(
        functools.partial(layer_kernel, n, head_size, cap),
        out_shape=jax.ShapeDtypeStruct((rows, width), BF),
        in_specs=[hbm] * 3 + [vmem] * 3 + [hbm] * 2 + [vmem] * 3 + [hbm] * 3,
        out_specs=vmem,
        scratch_shapes=[
            pltpu.VMEM((tokens, width_here), BF),
            pltpu.VMEM((pairs, hpp, tokens, LANES), BF),
            pltpu.VMEM((2 * reach + 2, chunks, 2, part_len, LANES), BF),
            pltpu.VMEM((SPLITS, side_rows, part_len), F32),
            pltpu.VMEM((n // 2 + 1, SPLITS, side_rows, part_len), F32),
            pltpu.VMEM((8, rows), jnp.int32),
            pltpu.VMEM((n // 2, 8, rows), jnp.int32),
            pltpu.VMEM((pairs, hpp, tokens, LANES), F32),
            pltpu.VMEM((pairs, hpp, tokens, LANES), F32),
            pltpu.VMEM((tp_count, rows, width_here), BF),
            pltpu.VMEM((tp_count, rows, width_here), BF),
            pltpu.VMEM((tp_count * width_here, width), BF),
            pltpu.VMEM((rows, width), F32),
            pltpu.VMEM((n // 2, rows, width), BF),
            pltpu.VMEM((n // 2, cap, width), BF),
            pltpu.VMEM((n, cap, width), BF),
            pltpu.VMEM((n, 4, cap, width), BF),
            pltpu.VMEM((width, hid), BF),
            pltpu.VMEM((width, hid), BF),
            pltpu.VMEM((hid, width), BF),
            pltpu.VMEM((4 * cap, hid), BF),
            pltpu.VMEM((n, 2, 2, cap, width), BF),
            pltpu.VMEM((n, 2, cap, width), BF),
            pltpu.VMEM((n, cap, width), BF),
            dma((3,)),
            dma((2 * chunks,)),
            dma((3,)),
        ]
        + [dma(((reach + 1) * chunks,)) for _ in range(4)]
        + [dma((n // 2 + 1,)) for _ in range(2)]
        + [dma((tp_count,)) for _ in range(2)]
        + [dma((n // 2,)) for _ in range(2)]
        + [dma((n,)) for _ in range(3)]
        + [dma((n // 2,)) for _ in range(2)]
        + [dma((n,)) for _ in range(12)],
        compiler_params=pltpu.CompilerParams(
            collective_id=1, has_side_effects=True, vmem_limit_bytes=VMEM_LIMIT
        ),
    )(
        queries,
        keys,
        values,
        cum_gate.T,
        documents[None, :],
        head_gain[None, :],
        out_weight,
        resid,
        norm_gain[None, :],
        routes.T,
        route_weights.T,
        w_gate[0],
        w_up[0],
        w_down[0],
    )


def solution(mesh):
    in_specs = (
        P("sp", "tp"),
        P("sp", "tp"),
        P("sp", "tp"),
        P("sp", "tp"),
        P("sp"),
        P("tp"),
        P(),
        P(("sp", "tp"), None),
        P(),
        P(("sp", "tp"), None),
        P(("sp", "tp"), None),
        P("sp", None, "tp"),
        P("sp", None, "tp"),
        P("sp", "tp", None),
    )
    out_specs = P(("sp", "tp"), None)
    return jax.shard_map(
        on_device, mesh=mesh, in_specs=in_specs, out_specs=out_specs, check_vma=False
    )
```

```python
import functools

import jax
import jax.numpy as jnp
from jax import lax
from jax.experimental import pallas as pl
from jax.experimental.pallas import tpu as pltpu
from jax.sharding import PartitionSpec as P

EPS = 1e-06
MESH = pl.DeviceIdType.MESH
NEG = -1e30
VMEM_LIMIT = 67043328
LANES = 128
SPLITS = 2
BF = jnp.bfloat16
F32 = jnp.float32


def layer_kernel(
    n,
    head_size,
    cap,
    q_hbm,
    k_hbm,
    v_hbm,
    gates_ref,
    docs_ref,
    gain_ref,
    wo_hbm,
    resid_hbm,
    norm_gain_ref,
    routes_ref,
    route_w_ref,
    wg_hbm,
    wu_hbm,
    wd_hbm,
    mixed_hbm,
    mixed_ref,
    q_in,
    qs,
    kv,
    aux_ref,
    aux_all,
    route_own,
    route_all,
    top,
    acc,
    normed,
    gathered,
    wo,
    wide,
    raw,
    crossing_rows,
    ret_ref,
    fan,
    wg,
    wu,
    wd,
    hidden,
    part,
    got,
    across,
    in_sem,
    kv_sem,
    w_sem,
    up_send,
    up_recv,
    over_send,
    over_recv,
    aux_send,
    aux_recv,
    h_send,
    h_recv,
    route_send,
    route_recv,
    rise_send,
    fall_send,
    raw_recv,
    y_send,
    y_recv,
    x_send,
    x_recv,
    c_send,
    c_recv,
    d_send,
    d_recv,
    p_send,
    p_recv,
    s_send,
    s_recv,
    r_send,
    r_recv,
):
    me = lax.axis_index("sp")
    t = lax.axis_index("tp")
    c, xi = lax.rem(t, 2), t // 2
    near = xi * 2 + (1 - c)
    far = (1 - xi) * 2 + c
    diag = 3 - t
    y, z = lax.rem(me, 2), me // 2
    floors, reach = n // 2, n // 4
    near_id = {"sp": me, "tp": near}
    far_id = {"sp": me, "tp": far}
    diag_id = {"sp": me, "tp": diag}
    mate_id = {"sp": me + 1 - 2 * y, "tp": t}
    above_id = {"sp": lax.rem(me + 2, n), "tp": t}
    below_id = {"sp": lax.rem(me + n - 2, n), "tp": t}

    tokens, width_here = q_in.shape
    pairs = width_here // LANES
    hpp = LANES // head_size
    keys = tokens // SPLITS
    chunks = pairs * SPLITS
    rows, width = mixed_ref.shape

    loads = [
        pltpu.make_async_copy(
            src.at[pl.ds(s * keys, keys), pl.ds(p * LANES, LANES)],
            kv.at[0, p * SPLITS + s, j],
            kv_sem.at[(p * SPLITS + s) * 2 + j],
        )
        for p in range(pairs)
        for s in range(SPLITS)
        for j, src in enumerate((k_hbm, v_hbm))
    ]
    q_load = pltpu.make_async_copy(q_hbm, q_in, in_sem.at[0])
    wo_load = pltpu.make_async_copy(wo_hbm, wo, in_sem.at[1])
    resid_load = pltpu.make_async_copy(resid_hbm, raw.at[z], in_sem.at[2])
    weights = [
        pltpu.make_async_copy(src, dst, w_sem.at[i])
        for i, (src, dst) in enumerate(((wg_hbm, wg), (wu_hbm, wu), (wd_hbm, wd)))
    ]
    for copy in loads:
        copy.start()
    q_load.start()

    heads = pairs * hpp
    for s in range(SPLITS):
        cols = slice(s * keys, (s + 1) * keys)
        doc_row = docs_ref[:, cols].astype(F32)
        aux_ref[s] = jnp.concatenate(
            [gates_ref[:, cols]] + [doc_row] * (aux_ref.shape[1] - heads), axis=0
        )
    route_own[...] = jnp.concatenate([routes_ref[...]] * 4, axis=0)

    barrier = pltpu.get_barrier_semaphore()

    def greet(k, carry):
        pl.semaphore_signal(
            barrier,
            inc=1,
            device_id={"sp": lax.rem(me + k, n), "tp": t},
            device_id_type=MESH,
        )
        return carry

    lax.fori_loop(1, n, greet, 0)
    for other in (near_id, far_id, diag_id):
        pl.semaphore_signal(barrier, inc=1, device_id=other, device_id_type=MESH)

    def remote(src, dst, send, recv, to):
        return pltpu.make_async_remote_copy(
            src_ref=src, dst_ref=dst, send_sem=send, recv_sem=recv, device_id=to, device_id_type=MESH
        )

    def up(d, i):
        return remote(
            kv.at[d, i],
            kv.at[d + 1, i],
            up_send.at[d * chunks + i],
            up_recv.at[d * chunks + i],
            above_id,
        )

    def over(d, i):
        return remote(
            kv.at[d, i],
            kv.at[reach + 1 + d, i],
            over_send.at[d * chunks + i],
            over_recv.at[d * chunks + i],
            mate_id,
        )

    def aux_copy(k):
        return remote(
            aux_ref,
            aux_all.at[k],
            aux_send.at[k],
            aux_recv.at[k],
            {"sp": lax.rem(me + k, n), "tp": t},
        )

    def rising(d):
        return (z + 1 < floors) & (z >= d) & (d < reach)

    def crossing(d):
        return (z >= d) & ((d > 0) | (y == 0)) & ((d < reach) | (y == 1))

    def coming(d):
        return (z >= d) & ((d > 0) | (y == 1)) & ((d < reach) | (y == 0))

    def forward(d, i):
        @pl.when(rising(d))
        def _():
            up(d, i).start()

        @pl.when(crossing(d))
        def _():
            over(d, i).start()

    pl.semaphore_wait(barrier, n + 2)

    def send_aux(k, carry):
        @pl.when(me + k < n)
        def _():
            aux_copy(k).start()

        return carry

    lax.fori_loop(1, n // 2 + 1, send_aux, 0)
    for copy in loads:
        copy.wait()
    lax.fori_loop(0, chunks, lambda i, z_: (forward(0, i), z_)[1], 0)

    def route_copy(b):
        return remote(
            route_own,
            route_all.at[z],
            route_send.at[b],
            route_recv.at[z],
            {"sp": 2 * b + y, "tp": t},
        )

    def route_in(b):
        return remote(route_own, route_all.at[b], route_send.at[b], route_recv.at[b], near_id)

    def send_route(b, carry):
        @pl.when(b != z)
        def _():
            route_copy(b).start()

        return carry

    lax.fori_loop(0, floors, send_route, 0)
    wo_load.start()
    resid_load.start()
    for copy in weights:
        copy.start()

    lane = lax.broadcasted_iota(jnp.int32, (1, LANES), 1)
    tile = min(tokens, 256)

    def mine(h):
        return (lane >= h * head_size) & (lane < (h + 1) * head_size)

    q_load.wait()
    for p in range(pairs):
        block = q_in[:, p * LANES : (p + 1) * LANES].astype(F32) * (head_size ** (-0.5))
        for h in range(hpp):
            qs[p, h] = jnp.where(mine(h), block, 0.0).astype(BF)
    top[...] = jnp.full(top.shape, NEG, F32)
    acc[...] = jnp.zeros(acc.shape, F32)

    def wider(x):
        return jnp.concatenate([x] * (keys // LANES), axis=1) if keys > LANES else x[:, :keys]

    def visit(slot, i, p, h, r0, bias, allowed):
        at = pl.ds(r0, tile)
        k = kv[slot, i, 0]
        v = jnp.where(mine(h), kv[slot, i, 1].astype(F32), 1.0).astype(BF)
        scores = lax.dot_general(
            qs[p, h, at, :], k, (((1,), (1,)), ((), ())), preferred_element_type=F32
        )
        scores = scores + bias
        if allowed is not None:
            scores = jnp.where(allowed, scores, NEG)
        before = top[p, h, at, :]
        highest = jnp.maximum(before, jnp.max(scores, axis=1, keepdims=True))
        exps = jnp.exp(scores - wider(highest))
        rescale = jnp.exp(before - highest)
        top[p, h, at, :] = highest
        acc[p, h, at, :] = acc[p, h, at, :] * rescale + jnp.dot(
            exps.astype(BF), v, preferred_element_type=F32
        )

    first_doc = aux_ref[0, heads : heads + 1, 0:1]
    spots_r = lax.broadcasted_iota(jnp.int32, (keys, keys), 0)
    spots_c = lax.broadcasted_iota(jnp.int32, (keys, keys), 1)
    doc_cols = [
        jnp.sum(
            jnp.where(spots_r == spots_c, aux_ref[s, heads : heads + 1, :], 0.0), axis=1, keepdims=True
        )
        for s in range(SPLITS)
    ]
    doc_col = jnp.concatenate(doc_cols, axis=0)

    def diagonal(p, carry):
        for s in range(SPLITS):
            i = p * SPLITS + s
            docs_here = aux_ref[s, heads : heads + 1, :]
            for h in range(hpp):
                gate_at = pl.ds(p * hpp + h, 1)
                bias = aux_ref[0, gate_at, :][:, 0:1] - aux_ref[s, gate_at, :]
                for r0 in range(0, tokens, tile):
                    if r0 + tile <= s * keys:
                        continue
                    key_pos = s * keys + lax.broadcasted_iota(jnp.int32, (1, keys), 1)
                    query_pos = r0 + lax.broadcasted_iota(jnp.int32, (tile, 1), 0)
                    allowed = (key_pos <= query_pos) & (
                        docs_here == doc_col[r0 : r0 + tile]
                    )
                    visit(0, i, p, h, r0, bias, allowed)
        return carry

    lax.fori_loop(0, pairs, diagonal, 0)
    shut = jnp.where(doc_col == first_doc, 0.0, 2e30)
    for p in range(pairs):
        for h in range(hpp):
            top[p, h] = jnp.where(shut > 0.0, 1e30, top[p, h])

    def earlier(slot, dist, i):
        p, s = i // SPLITS, lax.rem(i, SPLITS)
        same = aux_all[dist, s, heads : heads + 1, :] == first_doc
        for h in range(hpp):
            gate_at = pl.ds(p * hpp + h, 1)
            bias = jnp.where(
                same, aux_ref[0, gate_at, :][:, 0:1] - aux_all[dist, s, gate_at, :], NEG
            )
            for r0 in range(0, tokens, tile):
                visit(slot, i, p, h, r0, bias, None)

    def aux_here(k, i):
        @pl.when(i == 0)
        def _():
            aux_copy(k).wait_recv()

    def crossed(d, i):
        @pl.when(coming(d))
        def _():
            dist = 2 * d + 2 * y - 1
            aux_here(dist, i)
            over(d, i).wait_recv()
            earlier(reach + 1 + d, dist, i)

    def history(j, carry):
        d, i = j // chunks + 1, lax.rem(j, chunks)

        @pl.when(z >= d)
        def _():
            up(d - 1, i).wait_recv()
            forward(d, i)
            aux_here(2 * d, i)
            earlier(d, 2 * d, i)

        @pl.when(d >= 2)
        def _():
            crossed(d - 2, i)

        return carry

    wide_tile = 512 if width % 512 == 0 else width
    row_r = lax.broadcasted_iota(jnp.int32, (rows, rows), 0)
    row_c = lax.broadcasted_iota(jnp.int32, (rows, rows), 1)

    def column(row):
        return jnp.sum(jnp.where(row_r == row_c, row, 0.0), axis=1, keepdims=True)

    before_row = (row_r < row_c).astype(F32).astype(BF)
    slots = lax.broadcasted_iota(jnp.int32, (cap, 1), 0).astype(F32)

    def taken(routes, e):
        named = ((routes[0:1, :] == e) | (routes[1:2, :] == e)).astype(F32)
        spread_out = jnp.broadcast_to(named, (8, rows)).astype(BF)
        rank = jnp.dot(spread_out, before_row, preferred_element_type=F32)[0:1]
        return ((named > 0.0) & (rank == slots)).astype(F32).astype(BF)

    first_e, second_e = [column(routes_ref[r : r + 1, :].astype(F32)) for r in range(2)]
    lane_f = lane.astype(F32)
    named = ((first_e == lane_f) | (second_e == lane_f)).astype(F32)
    ranks = jnp.dot(
        (row_c < row_r).astype(F32).astype(BF), named.astype(BF), preferred_element_type=F32
    )
    wants = []
    for e in (first_e, second_e):
        rank = jnp.sum(jnp.where(e == lane_f, ranks, 0.0), axis=1, keepdims=True)
        wants.append(e * cap + rank)
    wants = jnp.concatenate(wants, axis=0)
    route_weights = [column(route_w_ref[r : r + 1, :]) for r in range(2)]

    lax.fori_loop(0, reach * chunks, history, 0)
    lax.fori_loop(0, chunks, lambda i, z_: (crossed(reach - 1, i), z_)[1], 0)
    lax.fori_loop(0, chunks, lambda i, z_: (crossed(reach, i), z_)[1], 0)

    def h_copy(q, to):
        return remote(normed.at[q], gathered.at[t], h_send.at[q], h_recv.at[t], to)

    def h_in(q):
        return remote(normed.at[q], gathered.at[q], h_send.at[q], h_recv.at[q], near_id)

    def settle(q):
        at = pl.ds(pl.multiple_of(q * rows, rows), rows)
        for p in range(pairs):
            total = None
            for h in range(hpp):
                state = acc[p, h, at, :]
                sums = pltpu.roll(state, head_size, 1)
                attended = jnp.where(mine(h), state / sums, 0.0)
                mean_square = jnp.sum(attended * attended, axis=1, keepdims=True) / head_size
                piece = attended * lax.rsqrt(mean_square + EPS)
                total = piece if total is None else total + piece
            cols = slice(p * LANES, (p + 1) * LANES)
            normed[q, :, cols] = (total * gain_ref[:, cols]).astype(BF)

    for q, to in ((far, far_id), (diag, diag_id), (near, near_id)):
        settle(q)
        h_copy(q, to).start()
    settle(t)

    wo_load.wait()
    resid_load.wait()

    def product(src, q, at):
        return jnp.dot(
            src,
            wo[pl.ds(pl.multiple_of(q * width_here, width_here), width_here), at : at + wide_tile],
            preferred_element_type=F32,
        )

    for at in range(0, width, wide_tile):
        wide[:, at : at + wide_tile] = product(normed[t], t, at)
    h_in(near).wait_recv()
    for at in range(0, width, wide_tile):
        wide[:, at : at + wide_tile] += product(gathered[near], near, at)
    h_in(far).wait_recv()
    h_in(diag).wait_recv()
    squares = jnp.zeros((rows, 1), F32)
    for at in range(0, width, wide_tile):
        cols = slice(at, at + wide_tile)
        value = (
            wide[:, cols]
            + product(gathered[far], far, at)
            + product(gathered[diag], diag, at)
            + raw[z, :, cols].astype(F32)
        )
        value = value.astype(BF).astype(F32)
        wide[:, cols] = value
        squares = squares + jnp.sum(value * value, axis=1, keepdims=True)
    scale = lax.rsqrt(squares / width + EPS)
    halves = 2
    half = width // halves

    def raw_part(b, h):
        return raw.at[b, :, pl.ds(h * half, half)]

    def carry_raw(b, h, send, to):
        return remote(
            raw_part(b, h), raw_part(b, h), send.at[b * halves + h], raw_recv.at[b * halves + h], to
        )

    def rise(b, h):
        return carry_raw(b, h, rise_send, above_id)

    def fall(b, h):
        return carry_raw(b, h, fall_send, below_id)

    def bring(b):
        @pl.when(b < z)
        def _():
            for h in range(halves):
                rise(b, h).wait_recv()

                @pl.when(z + 1 < floors)
                def _():
                    rise(b, h).start()

        @pl.when(b > z)
        def _():
            for h in range(halves):
                fall(b, h).wait_recv()

                @pl.when(z > 0)
                def _():
                    fall(b, h).start()

    inner = (z > 0) & (z + 1 < floors)

    @pl.when((z == 1) & inner)
    def _():
        bring(0)

    for h in range(halves):
        for at in range(h * half, (h + 1) * half, min(wide_tile, half)):
            cols = slice(at, at + min(wide_tile, half))
            raw[z, :, cols] = (wide[:, cols] * scale * norm_gain_ref[:, cols]).astype(BF)

        @pl.when(z + 1 < floors)
        def _():
            rise(z, h).start()

        @pl.when(z > 0)
        def _():
            fall(z, h).start()

    over_here = floors - 1 - z
    both_ways = jnp.maximum(jnp.minimum(z - 1, over_here), 0)

    def floor_at(j):
        turns = j - 1
        paired = turns <= 2 * both_ways
        step = jnp.where(paired, (turns + 1) // 2, turns - both_ways)
        up_next = jnp.where(paired, lax.rem(turns, 2) == 1, over_here > z - 1)
        mid = jnp.where(j == 1, 0, jnp.where(up_next, z + step, z - step))
        last = jnp.where(j == 1, z - 1, jnp.where(j == 2, 0, z + 1 - j))
        at = jnp.where(z == 0, j, jnp.where(over_here == 0, last, mid))
        return jnp.where(j == 0, z, at)

    def source(k):
        return 2 * floor_at(k // 2) + jnp.where(lax.rem(k, 2) == 0, y, 1 - y)

    def y_copy(b):
        return remote(
            crossing_rows.at[b], fan.at[2 * b + y, t], y_send.at[b], y_recv.at[b], mate_id
        )

    def y_in(b):
        return remote(
            crossing_rows.at[b], fan.at[2 * b + 1 - y, t], y_send.at[b], y_recv.at[b], mate_id
        )

    def select(b, routes):
        mate = me + 1 - 2 * y
        picks = jnp.concatenate([taken(routes, mate), taken(routes, me)], axis=0)
        for at in range(0, width, wide_tile):
            cols = slice(at, at + wide_tile)
            both = jnp.dot(picks, raw[b, :, cols], preferred_element_type=F32).astype(BF)
            crossing_rows[b, :, cols] = both[:cap]
            fan[2 * b + y, t, :, cols] = both[cap:]
        y_copy(b).start()

    def x_copy(k, q):
        p = source(k)
        return remote(fan.at[p, q], fan.at[p, q], x_send.at[p], x_recv.at[p], far_id)

    def c_copy(k, q):
        p = source(k)
        return remote(fan.at[p, q], fan.at[p, q], c_send.at[p], c_recv.at[p], near_id)

    def d_copy(k, q):
        p = source(k)
        return remote(fan.at[p, q], fan.at[p, q], d_send.at[p], d_recv.at[p], near_id)

    def p_copy(k):
        p = source(k)
        return remote(part.at[p, 1 - c], got.at[p], p_send.at[p], p_recv.at[p], near_id)

    def s_copy(k):
        p = source(k)
        return remote(part.at[p, c, 1 - xi], across.at[p], s_send.at[p], s_recv.at[p], far_id)

    def r_out(k):
        p = source(k)
        return remote(
            part.at[p, c, xi], ret_ref.at[me], r_send.at[p], r_recv.at[me], {"sp": p, "tp": t}
        )

    def r_in(p):
        return remote(part.at[p, c, xi], ret_ref.at[p], r_send.at[p], r_recv.at[p], near_id)

    def spread(k):
        x_copy(k, t).start()
        c_copy(k, t).start()

    def step_a(k):
        j = k // 2

        @pl.when(lax.rem(k, 2) == 0)
        def _():

            @pl.when(jnp.logical_not(inner))
            def _():
                bring(floor_at(j))

            @pl.when(inner & (j <= z) & (z > 1))
            def _():
                bring(jnp.where(j == 1, 0, z + 1 - j))

            route_in(floor_at(j)).wait_recv()
            select(floor_at(j), route_all[floor_at(j)])

        @pl.when(lax.rem(k, 2) == 1)
        def _():
            @pl.when(inner & (j >= 1) & (z + j < floors))
            def _():
                bring(z + j)

            y_in(floor_at(j)).wait_recv()

        spread(k)

    def step_x(k):
        x_copy(k, far).wait_recv()
        d_copy(k, far).start()

    def step_compute(k):
        p = source(k)
        c_copy(k, near).wait_recv()
        d_copy(k, diag).wait_recv()
        block = fan[p].reshape(4 * cap, width)
        gate = jnp.dot(block, wg[...], preferred_element_type=F32)
        up_ = jnp.dot(block, wu[...], preferred_element_type=F32)
        hidden[...] = (gate * jax.nn.sigmoid(gate) * up_).astype(BF)
        for at in range(0, width, wide_tile):
            down = jnp.dot(
                hidden[...], wd[:, at : at + wide_tile], preferred_element_type=F32
            ).astype(BF)
            for q in range(4):
                part[p, q % 2, q // 2, :, at : at + wide_tile] = down[q * cap : (q + 1) * cap]
        p_copy(k).start()

    def step_pair(k):
        p = source(k)
        p_copy(k).wait_recv()
        part[p, c, 1 - xi] = (
            part[p, c, 1 - xi].astype(F32) + got[p, 1 - xi].astype(F32)
        ).astype(BF)
        s_copy(k).start()

    def step_final(k):
        p = source(k)
        s_copy(k).wait_recv()
        total = (
            part[p, c, xi].astype(F32) + got[p, xi].astype(F32) + across[p].astype(F32)
        ).astype(BF)

        @pl.when(k == 0)
        def _():
            ret_ref[me] = total

        @pl.when(k > 0)
        def _():
            part[p, c, xi] = total
            r_out(k).start()

    select(z, routes_ref[...])
    spread(0)
    step_a(1)
    for k in (2, 3):
        step_a(k)
    for copy in weights:
        copy.wait()

    def turn(i):
        return jnp.where(i + 2 < n, i + 2, n - 1 - i)

    step_x(turn(0))

    def iteration(i, carry):
        @pl.when(i + 4 < n)
        def _():
            step_a(i + 4)

        @pl.when(i + 1 < n)
        def _():
            step_x(turn(i + 1))

        @pl.when(i >= 1)
        def _():
            step_pair(turn(i - 1))

        @pl.when(i < n)
        def _():
            step_compute(turn(i))

        @pl.when(i >= 2)
        def _():
            step_final(turn(i - 2))

        return carry

    lax.fori_loop(0, n + 1, iteration, 0)

    slot = lax.broadcasted_iota(jnp.int32, (1, cap), 1)

    def combine(p):
        picks = (wants == (p * cap + slot).astype(F32)).astype(F32).astype(BF)
        for at in range(0, width, wide_tile):
            cols = slice(at, at + wide_tile)
            chosen = jnp.dot(picks, ret_ref[p, :, cols], preferred_element_type=F32)
            wide[:, cols] += (
                route_weights[0] * chosen[:rows] + route_weights[1] * chosen[rows:]
            )

    def gather(i, carry):
        p = source(turn(i))
        r_in(p).wait_recv()
        combine(p)
        return carry

    lax.fori_loop(0, n - 2, gather, 0)
    step_final(0)
    combine(me)
    gather(n - 2, 0)
    mixed_ref[...] = wide[...].astype(BF)
    leave = pltpu.make_async_copy(mixed_ref, mixed_hbm, in_sem.at[0])
    leave.start()

    def sent_history(j, carry):
        d, i = j // chunks, lax.rem(j, chunks)

        @pl.when(rising(d))
        def _():
            up(d, i).wait_send()

        @pl.when(crossing(d))
        def _():
            over(d, i).wait_send()

        return carry

    lax.fori_loop(0, (reach + 1) * chunks, sent_history, 0)

    def sent_aux(k, carry):
        @pl.when(me + k < n)
        def _():
            aux_copy(k).wait_send()

        return carry

    lax.fori_loop(1, n // 2 + 1, sent_aux, 0)
    for q, to in ((far, far_id), (diag, diag_id), (near, near_id)):
        h_copy(q, to).wait_send()

    def sent_floor(b, carry):
        y_copy(b).wait_send()

        @pl.when(b != z)
        def _():
            route_copy(b).wait_send()

        for h in range(halves):
            @pl.when((b <= z) & (z + 1 < floors))
            def _():
                rise(b, h).wait_send()

            @pl.when((b >= z) & (z > 0))
            def _():
                fall(b, h).wait_send()

        return carry

    lax.fori_loop(0, floors, sent_floor, 0)

    def finish(k, carry):
        x_copy(k, t).wait_send()
        c_copy(k, t).wait_send()
        d_copy(k, far).wait_send()
        p_copy(k).wait_send()
        s_copy(k).wait_send()

        @pl.when(k > 0)
        def _():
            r_out(k).wait_send()

        return carry

    lax.fori_loop(0, n, finish, 0)
    leave.wait()


def on_device(
    queries,
    keys,
    values,
    cum_gate,
    documents,
    head_gain,
    out_weight,
    resid,
    norm_gain,
    routes,
    route_weights,
    w_gate,
    w_up,
    w_down,
):
    tokens, width_here = queries.shape
    heads_here = cum_gate.shape[1]
    head_size = width_here // heads_here
    n = lax.axis_size("sp")
    tp_count = lax.axis_size("tp")
    rows, width = resid.shape
    top_count = routes.shape[1]
    cap = 2 * top_count * tokens // (tp_count * n)
    hid = w_gate.shape[2]
    pairs, hpp = width_here // LANES, LANES // head_size
    part_len = tokens // SPLITS
    chunks = pairs * SPLITS
    reach = n // 4
    side_rows = -(-(heads_here + 1) // 8) * 8

    dma = pltpu.SemaphoreType.DMA
    hbm = pl.BlockSpec(memory_space=pl.ANY)
    vmem = pl.BlockSpec(memory_space=pltpu.VMEM)
    return pl.pallas_call(
        functools.partial(layer_kernel, n, head_size, cap),
        out_shape=jax.ShapeDtypeStruct((rows, width), BF),
        in_specs=[hbm] * 3 + [vmem] * 3 + [hbm] * 2 + [vmem] * 3 + [hbm] * 3,
        out_specs=hbm,
        scratch_shapes=[
            pltpu.VMEM((rows, width), BF),
            pltpu.VMEM((tokens, width_here), BF),
            pltpu.VMEM((pairs, hpp, tokens, LANES), BF),
            pltpu.VMEM((2 * reach + 2, chunks, 2, part_len, LANES), BF),
            pltpu.VMEM((SPLITS, side_rows, part_len), F32),
            pltpu.VMEM((n // 2 + 1, SPLITS, side_rows, part_len), F32),
            pltpu.VMEM((8, rows), jnp.int32),
            pltpu.VMEM((n // 2, 8, rows), jnp.int32),
            pltpu.VMEM((pairs, hpp, tokens, LANES), F32),
            pltpu.VMEM((pairs, hpp, tokens, LANES), F32),
            pltpu.VMEM((tp_count, rows, width_here), BF),
            pltpu.VMEM((tp_count, rows, width_here), BF),
            pltpu.VMEM((tp_count * width_here, width), BF),
            pltpu.VMEM((rows, width), F32),
            pltpu.VMEM((n // 2, rows, width), BF),
            pltpu.VMEM((n // 2, cap, width), BF),
            pltpu.VMEM((n, cap, width), BF),
            pltpu.VMEM((n, 4, cap, width), BF),
            pltpu.VMEM((width, hid), BF),
            pltpu.VMEM((width, hid), BF),
            pltpu.VMEM((hid, width), BF),
            pltpu.VMEM((4 * cap, hid), BF),
            pltpu.VMEM((n, 2, 2, cap, width), BF),
            pltpu.VMEM((n, 2, cap, width), BF),
            pltpu.VMEM((n, cap, width), BF),
            dma((3,)),
            dma((2 * chunks,)),
            dma((3,)),
        ]
        + [dma(((reach + 1) * chunks,)) for _ in range(4)]
        + [dma((n // 2 + 1,)) for _ in range(2)]
        + [dma((tp_count,)) for _ in range(2)]
        + [dma((n // 2,)) for _ in range(2)]
        + [dma((n,)) for _ in range(3)]
        + [dma((n // 2,)) for _ in range(2)]
        + [dma((n,)) for _ in range(12)],
        compiler_params=pltpu.CompilerParams(
            collective_id=1, has_side_effects=True, vmem_limit_bytes=VMEM_LIMIT
        ),
    )(
        queries,
        keys,
        values,
        cum_gate.T,
        documents[None, :],
        head_gain[None, :],
        out_weight,
        resid,
        norm_gain[None, :],
        routes.T,
        route_weights.T,
        w_gate[0],
        w_up[0],
        w_down[0],
    )


def solution(mesh):
    in_specs = (
        P("sp", "tp"),
        P("sp", "tp"),
        P("sp", "tp"),
        P("sp", "tp"),
        P("sp"),
        P("tp"),
        P(),
        P(("sp", "tp"), None),
        P(),
        P(("sp", "tp"), None),
        P(("sp", "tp"), None),
        P("sp", None, "tp"),
        P("sp", None, "tp"),
        P("sp", "tp", None),
    )
    out_specs = P(("sp", "tp"), None)
    return jax.shard_map(
        on_device, mesh=mesh, in_specs=in_specs, out_specs=out_specs, check_vma=False
    )
```
